32 devices in a mesh: ep: 8 (over z, x), tp: 4 (over y, core).
Axes of the slice: x: 2, y: 2, z: 4, core: 2. Of those that a mesh axis runs over, the one named last changes fastest.
Arguments:
- tokens: bfloat16 [4096, 2048], P(('ep', 'tp')), may hold values from -6 to 6
- routes: int32 [4096, 2], P(('ep', 'tp')), may hold values from 0 to 31, as said below
- gates: float32 [4096, 2], P(('ep', 'tp')), may hold values from 0.1 to 0.6
- w_gate: bfloat16 [32, 2048, 768], P(('ep', 'tp')), may hold values from -0.125 to 0.125
- w_up: bfloat16 [32, 2048, 768], P(('ep', 'tp')), may hold values from -0.125 to 0.125
- w_down: bfloat16 [32, 768, 2048], P(('ep', 'tp')), may hold values from -0.21875 to 0.21875
- moe_out: bfloat16 [4096, 2048], P('ep', 'tp'), may hold values from -16 to 16
- norm_gain: float32 [2048], P('tp'), may hold values from 0.1 to 1.9
- out_grad: bfloat16 [4096, 2048], P('ep', 'tp'), may hold values from -16 to 16
Outputs:
- token_grad: bfloat16 [4096, 2048], P(('ep', 'tp'))
- gates_grad: bfloat16 [4096, 2], P(('ep', 'tp'))
- w_gate_grad: bfloat16 [32, 2048, 768], P(('ep', 'tp'))
- w_up_grad: bfloat16 [32, 2048, 768], P(('ep', 'tp'))
- w_down_grad: bfloat16 [32, 768, 2048], P(('ep', 'tp'))
The draws below stay inside these ranges and needn't reach their ends.
Inputs may be any that keep to these rules, and one draw needn't show every extreme that they name: `routes`: the two experts of a row differ and lie in one group (expert e is in group e // 8). In the 128 rows of one device the tokens fall into the groups in shares 3/8, 3/8, 1/8, 1/8 of 128, which group takes which share varying. In the rows of one device no expert is named more than 16 times, and one expert is named exactly 16 times in the rows of every device.
All inputs are finite; a program needn't handle non-finite values.
Results may differ from the reference program's by a relative error of at most 0.0071.
Values may be sent and summed in bfloat16 or wider, within the bound.
A program may use at most 128 MiB of HBM per device.

```python
import jax
import jax.numpy as jnp
from jax import lax

D = 2048
F = 768
GROUPS = 4
TOPK = 2
TOK_DEV = 128
EXPERTS = 32
EXP_GROUP = 8
CAP = 16
TOKENS = 4096


def draw_routes(key, part):
    tickets = EXP_GROUP * CAP
    shares = [3 * TOK_DEV // 8, 3 * TOK_DEV // 8, TOK_DEV // 8, TOK_DEV // 8]
    hot_global = jax.random.randint(jax.random.fold_in(key, 11), (), 0, EXPERTS)

    def one_block(block_key):
        sub_keys = jax.random.split(block_key, 4)
        group_order = jax.random.permutation(sub_keys[0], GROUPS)
        token_order = jax.random.permutation(sub_keys[1], TOK_DEV)
        hot_inner = jax.random.randint(sub_keys[2], (GROUPS,), 0, EXP_GROUP)
        noise_draw = jax.random.randint(sub_keys[3], (GROUPS, tickets), 0, 2 ** 19)
        ticket_ids = jnp.arange(tickets, dtype=jnp.int32)
        inner_ids = ticket_ids // CAP
        result = jnp.zeros((TOK_DEV, 2), jnp.int32)
        offset = 0
        for rank in range(GROUPS):
            expert_ids = group_order[rank] * EXP_GROUP + inner_ids
            hot_flag = jnp.logical_or(inner_ids == hot_inner[rank], expert_ids == hot_global).astype(jnp.int32)
            score_value = (hot_flag * 2 ** 19 + noise_draw[rank]) * tickets + ticket_ids
            share_size = shares[rank]
            picked = lax.top_k(score_value, 2 * share_size)[1]
            chosen = jnp.sort(expert_ids[picked])
            places = token_order[offset:offset + share_size]
            result = result.at[places, 0].set(chosen[:share_size])
            result = result.at[places, 1].set(chosen[share_size:])
            offset = offset + share_size
        return result
    block_keys = jax.random.split(jax.random.fold_in(key, 12), TOKENS // TOK_DEV)
    return jax.vmap(one_block)(block_keys).reshape(TOKENS, 2).astype(jnp.int32)


def paired_fields(key):
    sub_keys = jax.random.split(jax.random.fold_in(key, 21), 5)
    base = jax.random.normal(sub_keys[0], (TOKENS, D), jnp.float32)
    block_scale = jnp.exp(jax.random.uniform(sub_keys[1], (8,), jnp.float32, -1.2, 1.2))
    fine_scale = jnp.exp(jax.random.uniform(sub_keys[2], (D,), jnp.float32, -0.35, 0.35))
    columns = jnp.arange(D) * 8 // D
    col_scale = block_scale[columns] * fine_scale
    saved_out = jnp.clip(base * col_scale[None, :], -16.0, 16.0)
    noise_part = jax.random.normal(sub_keys[4], (TOKENS, D), jnp.float32)
    cotangent = jnp.clip(0.6 * base + 0.8 * noise_part, -16.0, 16.0)
    return (saved_out, cotangent)


def draw_moe_out(key, part):
    return paired_fields(key)[0].astype(jnp.bfloat16)


def draw_out_grad(key, part):
    return paired_fields(key)[1].astype(jnp.bfloat16)


def steps_of(key, shape, pieces, smallest, high):
    def one(dim, parts):
        draws = jax.random.uniform(jax.random.fold_in(jax.random.fold_in(key, 6), dim), (parts,), jnp.float32, smallest / len(pieces), high / len(pieces))
        return jnp.repeat(jnp.exp(draws), shape[dim] // parts).reshape((-1,) + (1,) * (len(shape) - dim - 1))

    loudness = one(*pieces[0])
    for cut in pieces[1:]:
        loudness = loudness * one(*cut)
    return loudness


def gaussian(key, extent, deviation, limit, shards=(), held_as=jnp.bfloat16):
    values = deviation * jax.random.normal(key, extent, jnp.float32)
    if shards:
        values = values * steps_of(key, extent, shards, -0.22, 0.18)
    return jnp.clip(values, -limit, limit).astype(held_as)


def setup_inputs(seed: int = 0) -> dict:
    arg_keys = jax.random.split(jax.random.key(seed), 10)
    tokens = gaussian(arg_keys[0], (TOKENS, D), 1.0, 6.0, ((0, 32),))
    routes = draw_routes(jax.random.fold_in(arg_keys[9], 71), 0)
    gates = jnp.clip(0.1 + 0.5 * jax.random.uniform(arg_keys[2], (TOKENS, TOPK), jnp.float32) ** steps_of(arg_keys[2], (TOKENS, TOPK), ((0, 32),), -0.2, 0.2), 0.1, 0.6)
    w_gate = gaussian(arg_keys[3], (EXPERTS, D, F), D ** -0.5, 0.125, ((0, 32),))
    w_up = gaussian(arg_keys[4], (EXPERTS, D, F), D ** -0.5, 0.125, ((0, 32),))
    w_down = gaussian(arg_keys[5], (EXPERTS, F, D), F ** -0.5, 0.21875, ((0, 32),))
    moe_out = draw_moe_out(jax.random.fold_in(arg_keys[9], 71), 0)
    norm_gain = jnp.clip(1.0 + 0.18 * jax.random.normal(arg_keys[7], (D,), jnp.float32), 0.1, 1.9)
    out_grad = draw_out_grad(jax.random.fold_in(arg_keys[9], 71), 0)
    return {"tokens": tokens, "routes": routes, "gates": gates, "w_gate": w_gate, "w_up": w_up, "w_down": w_down, "moe_out": moe_out, "norm_gain": norm_gain, "out_grad": out_grad}


epsilon = 1e-06
block_rows = 256

def contract(left, right, left_dim, right_dim):
    return lax.dot_general(left, right, (((left_dim,), (right_dim,)), ((), ())), preferred_element_type=jnp.float32)

def norm_backward(moe_out, norm_gain, out_grad):
    features = moe_out.shape[1]
    saved_out = moe_out.astype(jnp.float32)
    scaled = norm_gain.astype(jnp.float32)[None, :] * out_grad.astype(jnp.float32)
    square_sum = lax.optimization_barrier(jnp.sum(saved_out * saved_out, axis=1))
    cross_sum = lax.optimization_barrier(jnp.sum(saved_out * scaled, axis=1))
    inv_rms = lax.rsqrt(square_sum / features + epsilon)
    result = inv_rms[:, None] * scaled - saved_out * (inv_rms ** 3 * cross_sum / features)[:, None]
    return result.astype(jnp.bfloat16)

def expert_terms(row_block, cot_block, gate_row, w_gate_one, w_up_one, w_down_one):
    pre_gate = jnp.dot(row_block, w_gate_one, preferred_element_type=jnp.float32)
    pre_up = jnp.dot(row_block, w_up_one, preferred_element_type=jnp.float32)
    sigmoid_gate = jax.nn.sigmoid(pre_gate)
    activated = pre_gate * sigmoid_gate
    hidden = activated * pre_up
    hid_grad = contract(cot_block, w_down_one, 1, 1)
    gate_grad = lax.optimization_barrier(jnp.sum(hidden * hid_grad, axis=1)).astype(jnp.bfloat16)
    weight = gate_row.astype(jnp.float32)[:, None]
    d_hidden = weight * hid_grad
    d_gate = (d_hidden * pre_up * sigmoid_gate * (1.0 + pre_gate * (1.0 - sigmoid_gate))).astype(jnp.bfloat16)
    d_up = (d_hidden * activated).astype(jnp.bfloat16)
    token_back = (contract(d_gate, w_gate_one, 1, 1) + contract(d_up, w_up_one, 1, 1)).astype(jnp.bfloat16)
    scaled_cot = (weight * cot_block.astype(jnp.float32)).astype(jnp.bfloat16)
    grad_gate = contract(row_block, d_gate, 0, 0)
    grad_up = contract(row_block, d_up, 0, 0)
    grad_down = contract(hidden.astype(jnp.bfloat16), scaled_cot, 0, 0)
    return (token_back, gate_grad, grad_gate, grad_up, grad_down)

def reference(tokens, routes, gates, w_gate, w_up, w_down, moe_out, norm_gain, out_grad):
    features = tokens.shape[1]
    hidden_width = w_gate.shape[2]
    expert_cot = norm_backward(moe_out, norm_gain, out_grad)
    flat_ids = routes.reshape(-1).astype(jnp.int32)
    route_count = flat_ids.shape[0]
    flat_token = (jnp.arange(route_count, dtype=jnp.int32) // TOPK).astype(jnp.int32)
    flat_gate = gates.reshape(-1).astype(jnp.bfloat16)
    sorted_order = jnp.argsort(flat_ids, stable=True).astype(jnp.int32)
    totals = jnp.zeros((EXPERTS,), jnp.int32).at[flat_ids].add(1)
    starts = (jnp.cumsum(totals) - totals).astype(jnp.int32)
    token_pad = jnp.concatenate([tokens, jnp.zeros((1, features), jnp.bfloat16)], axis=0)
    cot_pad = jnp.concatenate([expert_cot, jnp.zeros((1, features), jnp.bfloat16)], axis=0)

    def per_expert(state_pair, inputs):
        expert_index, w_gate_one, w_up_one, w_down_one = inputs
        first_slot = starts[expert_index]
        load_size = totals[expert_index]

        def one_block(block_index, state):
            route_dx, route_gg, acc_gate, acc_up, acc_down = state
            position = (first_slot + block_index * block_rows + jnp.arange(block_rows, dtype=jnp.int32)).astype(jnp.int32)
            in_range = position < first_slot + load_size
            route_ids = sorted_order[jnp.clip(position, 0, route_count - 1)]
            token_ids = jnp.where(in_range, flat_token[route_ids], TOKENS).astype(jnp.int32)
            gate_row = jnp.where(in_range, flat_gate[route_ids], jnp.zeros((), jnp.bfloat16))
            target = jnp.where(in_range, route_ids, route_count).astype(jnp.int32)
            token_back, gate_grad, grad_gate, grad_up, grad_down = expert_terms(token_pad[token_ids], cot_pad[token_ids], gate_row, w_gate_one, w_up_one, w_down_one)
            route_dx = route_dx.at[target].set(token_back)
            route_gg = route_gg.at[target].set(gate_grad)
            return (route_dx, route_gg, acc_gate + grad_gate, acc_up + grad_up, acc_down + grad_down)
        blocks = (load_size + block_rows - 1) // block_rows
        start_state = (state_pair[0], state_pair[1], jnp.zeros((features, hidden_width), jnp.float32), jnp.zeros((features, hidden_width), jnp.float32), jnp.zeros((hidden_width, features), jnp.float32))
        route_dx, route_gg, acc_gate, acc_up, acc_down = lax.fori_loop(0, blocks, one_block, start_state)
        return ((route_dx, route_gg), (acc_gate.astype(jnp.bfloat16), acc_up.astype(jnp.bfloat16), acc_down.astype(jnp.bfloat16)))
    start_pair = (jnp.zeros((route_count + 1, features), jnp.bfloat16), jnp.zeros((route_count + 1,), jnp.bfloat16))
    final_pair, stacked = lax.scan(per_expert, start_pair, (jnp.arange(EXPERTS, dtype=jnp.int32), w_gate, w_up, w_down))
    route_dx, route_gg = final_pair
    token_grad = lax.optimization_barrier(jnp.sum(route_dx[:route_count].astype(jnp.float32).reshape(TOKENS, TOPK, features), axis=1)).astype(jnp.bfloat16)
    gates_grad = route_gg[:route_count].reshape(TOKENS, TOPK)
    return (token_grad, gates_grad, stacked[0], stacked[1], stacked[2])
```

```python
import functools

import jax
import jax.numpy as jnp
from jax import lax
from jax.experimental import pallas as pl
from jax.experimental.pallas import tpu as pltpu
from jax.sharding import Mesh
from jax.sharding import PartitionSpec as P

epsilon = 1e-06
groups = 4
MESH = pl.DeviceIdType.MESH
AXES = ("z", "x", "tp")
META_ROWS = 8
LANES = 128


def contract(left, right, left_dim, right_dim, **kw):
    return lax.dot_general(
        left, right, (((left_dim,), (right_dim,)), ((), ())), preferred_element_type=jnp.float32, **kw
    )


def earlier_equal(ids):
    count = ids.shape[-1]
    place = jnp.arange(count, dtype=jnp.int32)
    same = (ids[..., :, None] == ids[..., None, :]) & (place[:, None] > place[None, :])
    return jnp.sum(same.astype(jnp.int32), axis=-1)


class Place:
    def __init__(self, plane_size):
        self.z, self.x, self.t = (lax.axis_index(name) for name in AXES)
        self.zc, self.tc = lax.axis_size("z"), lax.axis_size("tp")
        self.plane = plane_size
        self.own = self.x * self.tc + self.t

    def at(self, d, k=0):
        return (lax.rem(self.z + d, self.zc), self.x, lax.rem(self.t + k, self.tc))

    def back(self, d):
        return (lax.rem(self.z + self.zc - d, self.zc), self.x, self.t)

    def peer(self, k):
        q = lax.rem(self.own + k, self.plane)
        return q, (self.z, q // self.tc, lax.rem(q, self.tc))


def enter(place, wide):
    barrier = pltpu.get_barrier_semaphore()

    def greet(device):
        pl.semaphore_signal(barrier, inc=1, device_id=device, device_id_type=MESH)

    lax.fori_loop(1, place.plane, lambda k, c: (greet(place.peer(k)[1]), c)[1], 0)
    across = place.tc if wide else 1
    for d in range(1, place.zc):
        lax.fori_loop(0, across, lambda k, c: (greet(place.at(d, k)), c)[1], 0)
    pl.semaphore_wait(barrier, place.plane - 1 + (place.zc - 1) * across)


def each(first, last, act):
    lax.fori_loop(first, last, lambda k, c: (act(k), c)[1], 0)


def columns(features, act):
    chunk = min(512, features)
    each(0, features // chunk, lambda c: act(pl.ds(pl.multiple_of(c * chunk, chunk), chunk)))


def iota(shape, dim):
    return lax.broadcasted_iota(jnp.int32, shape, dim)


def chosen(meta, row, slots, width):
    ids = meta[row : row + 1, :width].astype(jnp.int32)
    return iota((slots, width), 0) == ids


def picker(meta, slots, width):
    return (chosen(meta, 0, slots, width) | chosen(meta, 1, slots, width)).astype(
        jnp.float32
    ).astype(jnp.bfloat16)


def dispatch_kernel(
    plane_size, slots, tok_ref, meta_ref, saved_ref, grad_ref, gain_ref,
    tok_out, cot_out, w_out, meta_out,
    mbuf, stat, stbuf, cotz, ztok, zcot, stok, scot, wsend, wrecv,
    ms_sem, mr_sem, ss_sem, sr_sem, zs_sem, zr_sem, ps_sem, pr_sem, loc_sem, ws_sem, wr_sem,
):
    place = Place(plane_size)
    z, x, t, zc, tc = place.z, place.x, place.t, place.zc, place.tc
    own, peer = place.own, place.peer
    features = tok_ref.shape[-1]
    group_rows = tok_ref.shape[1]
    part = saved_ref.shape[-1]
    block = saved_ref.shape[0] // tc
    all_slots = plane_size * slots
    bf16 = jnp.bfloat16
    enter(place, True)

    def rows_of(q):
        return pl.ds(pl.multiple_of(q * slots, slots), slots)

    def remote(src, dst, send, recv, device):
        return pltpu.make_async_remote_copy(
            src_ref=src, dst_ref=dst, send_sem=send, recv_sem=recv, device_id=device, device_id_type=MESH
        )

    def meta_copy(d, k):
        return remote(
            meta_ref.at[lax.rem(z + d, zc)], mbuf.at[d, t], ms_sem.at[d, k], mr_sem.at[d, k], place.at(d, k)
        )

    def stat_copy(k):
        return remote(stat, stbuf.at[k], ss_sem.at[k], sr_sem.at[k], place.at(0, k))

    def z_copy(a, d):
        src, dst = ((tok_ref, ztok), (cotz, zcot))[a]
        return remote(
            src.at[lax.rem(z + d, zc)], dst.at[d], zs_sem.at[a, d], zr_sem.at[a, d], place.at(d)
        )

    def plane_parts(a, d, q):
        if a == 0:
            return stok.at[d, rows_of(q)], tok_out.at[d, rows_of(own)]
        cols = pl.ds(pl.multiple_of(t * part, part), part)
        return scot.at[d, :, rows_of(q)], cot_out.at[d, x, :, :, cols]

    def plane_copy(a, d, k):
        q, device = peer(k)
        src, dst = plane_parts(a, d, q)
        return remote(src, dst, ps_sem.at[a, d, k], pr_sem.at[a, d, k], device)

    def own_copy(a, d):
        src, dst = plane_parts(a, d, own)
        return pltpu.make_async_copy(src, dst, loc_sem.at[a, d])

    def w_copy(k):
        q, device = peer(k)
        return remote(wsend.at[rows_of(q)], wrecv.at[rows_of(own)], ws_sem.at[k], wr_sem.at[k], device)

    def spread_out(a, d):
        each(1, plane_size, lambda k: plane_copy(a, d, k).start())
        own_copy(a, d).start()

    def send_tok(d):
        sel = picker(mbuf[d, t], all_slots, group_rows)

        def one(cols):
            rows = ztok[d, :, cols] if d else tok_ref[z, :, cols]
            stok[d, :, cols] = jnp.dot(sel, rows, preferred_element_type=jnp.float32).astype(bf16)

        columns(features, one)
        spread_out(0, d)

    def send_cot(d):
        for b in range(tc):
            sel = picker(mbuf[d, b], all_slots, group_rows)
            rows = slice(b * group_rows, (b + 1) * group_rows)
            value = zcot[d, rows, :] if d else cotz[z, rows, :]
            scot[d, b] = jnp.dot(sel, value, preferred_element_type=jnp.float32).astype(bf16)
        spread_out(1, d)

    mbuf[0, t] = meta_ref[z]
    for d in range(zc):
        each(0 if d else 1, tc, lambda k: meta_copy(d, k).start())
    for d in range(1, zc):
        z_copy(0, d).start()

    eye = iota((block, block), 0) == iota((block, block), 1)
    gain = gain_ref[...]
    for b in range(tc):
        rows = slice(b * block, (b + 1) * block)
        saved = saved_ref[rows, :].astype(jnp.float32)
        scaled = gain * grad_ref[rows, :].astype(jnp.float32)
        for i, value in enumerate((saved * saved, saved * scaled)):
            total = jnp.sum(value, axis=1, keepdims=True)
            row = i * tc + b
            stat[row : row + 1, :] = jnp.sum(jnp.where(eye, total, 0.0), axis=0, keepdims=True)
    each(1, tc, lambda k: stat_copy(k).start())

    send_tok(0)

    each(1, tc, lambda k: stat_copy(k).wait_recv())
    each(1, tc, lambda k: meta_copy(0, k).wait_recv())
    totals = stat[...]
    for k in range(1, tc):
        totals = totals + stbuf[k]
    inv = lax.rsqrt(totals[:tc] / features + epsilon)
    coef = inv * inv * inv * totals[tc:] / features
    for b in range(tc):
        rows = slice(b * block, (b + 1) * block)
        saved = saved_ref[rows, :].astype(jnp.float32)
        scaled = gain * grad_ref[rows, :].astype(jnp.float32)
        inv_col = jnp.sum(jnp.where(eye, inv[b : b + 1], 0.0), axis=1, keepdims=True)
        coef_col = jnp.sum(jnp.where(eye, coef[b : b + 1], 0.0), axis=1, keepdims=True)
        cot = (inv_col * scaled - saved * coef_col).astype(bf16)
        pack = chosen(mbuf[0, b], 4, zc * group_rows, block).astype(jnp.float32).astype(bf16)
        packed = jnp.dot(pack, cot, preferred_element_type=jnp.float32).astype(bf16)
        for g in range(zc):
            cotz[g, b * group_rows : (b + 1) * group_rows, :] = packed[g * group_rows : (g + 1) * group_rows]
    for d in range(1, zc):
        z_copy(1, d).start()
    send_cot(0)

    for d in range(1, zc):
        each(0, tc, lambda k: meta_copy(d, k).wait_recv())
    weights = jnp.zeros((all_slots, LANES), jnp.float32)
    for d in range(zc):
        meta = mbuf[d, t]
        meta_out[d] = meta
        total = jnp.zeros((all_slots, 1), jnp.float32)
        for i in range(2):
            hit = chosen(meta, i, all_slots, group_rows)
            total = total + jnp.sum(
                jnp.where(hit, meta[2 + i : 3 + i, :group_rows], 0.0), axis=1, keepdims=True
            )
        weights = jnp.where(iota((all_slots, LANES), 1) == d, total, weights)
    wsend[...] = weights.astype(bf16)
    each(1, plane_size, lambda k: w_copy(k).start())
    wrecv[rows_of(own)] = wsend[rows_of(own)]

    for d in range(1, zc):
        z_copy(0, d).wait_recv()
        send_tok(d)
    for d in range(1, zc):
        z_copy(1, d).wait_recv()
        send_cot(d)

    each(1, plane_size, lambda k: w_copy(k).wait_recv())
    w_out[...] = wrecv[...]
    for a in range(2):
        for d in range(zc):
            own_copy(a, d).wait()
            each(1, plane_size, lambda k: plane_copy(a, d, k).wait(), )
            if d:
                z_copy(a, d).wait_send()
    for d in range(zc):
        each(0 if d else 1, tc, lambda k: meta_copy(d, k).wait_send())
    each(1, tc, lambda k: stat_copy(k).wait_send())
    each(1, plane_size, lambda k: w_copy(k).wait_send())


def combine_kernel(
    plane_size, slots, back_ref, gg_ref, meta_ref, out_ref, gout_ref,
    rbuf, cbuf, ggbuf, gbuf, gland, zs_sem, zr_sem, ps_sem, pr_sem, loc_sem, own_sem,
    gs_sem, gr_sem, gzs_sem, gzr_sem,
):
    place = Place(plane_size)
    z, zc, own, peer = place.z, place.zc, place.own, place.peer
    features = back_ref.shape[-1]
    group_rows = out_ref.shape[1]
    all_slots = plane_size * slots
    enter(place, False)

    def rows_of(q):
        return pl.ds(pl.multiple_of(q * slots, slots), slots)

    def remote(src, dst, send, recv, device):
        return pltpu.make_async_remote_copy(
            src_ref=src, dst_ref=dst, send_sem=send, recv_sem=recv, device_id=device, device_id_type=MESH
        )

    def plane_copy(d, k):
        q, device = peer(k)
        return remote(
            back_ref.at[d, rows_of(q)], rbuf.at[d, rows_of(own)], ps_sem.at[d, k], pr_sem.at[d, k], device
        )

    def own_rows(d):
        return pltpu.make_async_copy(back_ref.at[d, rows_of(own)], rbuf.at[d, rows_of(own)], loc_sem.at[d])

    def gg_copy(k):
        q, device = peer(k)
        return remote(gg_ref.at[rows_of(q)], ggbuf.at[rows_of(own)], gs_sem.at[k], gr_sem.at[k], device)

    def z_copy(d):
        return remote(cbuf.at[d], out_ref.at[z], zs_sem.at[d], zr_sem.at[d], place.back(d))

    def gz_copy(d):
        return remote(gbuf.at[d], gland.at[z], gzs_sem.at[d], gzr_sem.at[d], place.back(d))

    keep = pltpu.make_async_copy(cbuf.at[0], out_ref.at[z], own_sem)
    order = list(range(1, zc)) + [0]
    each(1, plane_size, lambda k: gg_copy(k).start())
    ggbuf[rows_of(own)] = gg_ref[rows_of(own)]
    for d in order:
        own_rows(d).start()
        each(1, plane_size, lambda k: plane_copy(d, k).start())
    each(1, plane_size, lambda k: gg_copy(k).wait_recv())
    returned = ggbuf[...].astype(jnp.float32)
    for d in order:
        meta = meta_ref[d]
        column = jnp.sum(
            jnp.where(iota(returned.shape, 1) == d, returned, 0.0), axis=1, keepdims=True
        )
        for i in range(2):
            hit = chosen(meta, i, all_slots, LANES)
            gbuf[d, i : i + 1, :] = jnp.sum(jnp.where(hit, column, 0.0), axis=0, keepdims=True)
        if d:
            gz_copy(d).start()
        else:
            gland[z] = gbuf[0]
    for d in order:
        own_rows(d).wait()
        each(1, plane_size, lambda k: plane_copy(d, k).wait_recv())
        sel = picker(meta_ref[d], all_slots, group_rows)

        def one(cols):
            cbuf[d, :, cols] = contract(sel, rbuf[d, :, cols], 0, 0).astype(cbuf.dtype)

        columns(features, one)
        if d:
            z_copy(d).start()
        else:
            keep.start()
    for d in order:
        each(1, plane_size, lambda k: plane_copy(d, k).wait_send())
        if d:
            gz_copy(d).wait()
            z_copy(d).wait()
    keep.wait()
    gout_ref[...] = gland[...]
    each(1, plane_size, lambda k: gg_copy(k).wait_send())


def vmem():
    return pl.BlockSpec(memory_space=pltpu.VMEM)


def anywhere():
    return pl.BlockSpec(memory_space=pl.ANY)


def dispatch(tok_send, meta, saved, grad, gain, plane_size, slots, tc):
    zc, group_rows, features = tok_send.shape
    part = saved.shape[1]
    rows = plane_size * slots
    bf16 = tok_send.dtype
    dma, struct, space = pltpu.SemaphoreType.DMA, jax.ShapeDtypeStruct, pltpu.VMEM
    f32 = jnp.float32
    return pl.pallas_call(
        functools.partial(dispatch_kernel, plane_size, slots),
        out_shape=(
            struct((zc, rows, features), bf16),
            struct((zc, plane_size // tc, tc, slots, features), bf16),
            struct((rows, LANES), bf16),
            struct(meta.shape, f32),
        ),
        in_specs=[vmem()] * 5,
        out_specs=(anywhere(), anywhere(), vmem(), vmem()),
        scratch_shapes=[
            space((zc, tc, META_ROWS, LANES), f32),
            space((2 * tc, LANES), f32),
            space((tc, 2 * tc, LANES), f32),
            space((zc, tc * group_rows, part), bf16),
            space((zc, group_rows, features), bf16),
            space((zc, tc * group_rows, part), bf16),
            space((zc, rows, features), bf16),
            space((zc, tc, rows, part), bf16),
            space((rows, LANES), bf16),
            space((rows, LANES), bf16),
            dma((zc, tc)),
            dma((zc, tc)),
            dma((tc,)),
            dma((tc,)),
            dma((2, zc)),
            dma((2, zc)),
            dma((2, zc, plane_size)),
            dma((2, zc, plane_size)),
            dma((2, zc)),
            dma((plane_size,)),
            dma((plane_size,)),
        ],
        compiler_params=pltpu.CompilerParams(
            collective_id=0, has_side_effects=True, vmem_limit_bytes=48 * 1024 * 1024
        ),
        name="dispatch",
    )(tok_send, meta, saved, grad, gain)


def combine(back, gg, meta, group_rows, plane_size, slots):
    zc, rows, features = back.shape
    dma, struct, space = pltpu.SemaphoreType.DMA, jax.ShapeDtypeStruct, pltpu.VMEM
    return pl.pallas_call(
        functools.partial(combine_kernel, plane_size, slots),
        out_shape=(struct((zc, group_rows, features), back.dtype), struct(meta.shape, meta.dtype)),
        in_specs=[anywhere(), vmem(), vmem()],
        out_specs=(anywhere(), vmem()),
        scratch_shapes=[
            space(back.shape, back.dtype),
            space((zc, group_rows, features), back.dtype),
            space(gg.shape, gg.dtype),
            space(meta.shape, meta.dtype),
            space(meta.shape, meta.dtype),
            dma((zc,)),
            dma((zc,)),
            dma((zc, plane_size)),
            dma((zc, plane_size)),
            dma((zc,)),
            dma(()),
            dma((plane_size,)),
            dma((plane_size,)),
            dma((zc,)),
            dma((zc,)),
        ],
        compiler_params=pltpu.CompilerParams(
            collective_id=1, has_side_effects=True, vmem_limit_bytes=48 * 1024 * 1024
        ),
        name="combine",
    )(back, gg, meta)


def local(tokens, routes, gates, w_gate, w_up, w_down, moe_out, norm_gain, out_grad):
    z_count, x_count, t_count = (lax.axis_size(name) for name in AXES)
    plane_size = x_count * t_count
    devices = z_count * plane_size
    tok_rows, features = tokens.shape
    top_count = routes.shape[1]
    capacity = groups * tok_rows // devices
    slots = -(-capacity // 16) * 16
    group_rows = 3 * tok_rows // 8
    rows = plane_size * slots
    bf16, f32 = jnp.bfloat16, jnp.float32

    own_ids = routes.T.reshape(-1)
    own_group = routes[:, 0] // plane_size
    z_slot = own_group * group_rows + earlier_equal(own_group)
    hit = jnp.arange(groups * group_rows, dtype=jnp.int32)[:, None] == z_slot[None, :]
    tok_send = jnp.dot(hit.astype(bf16), tokens, preferred_element_type=f32).astype(bf16)
    slot_of = (own_ids % plane_size) * slots + earlier_equal(own_ids)
    values = jnp.concatenate(
        [
            slot_of.reshape(top_count, tok_rows).astype(f32) + 1.0,
            gates.T.astype(bf16).astype(f32),
        ]
    )
    packed = contract(values, hit.astype(f32), 1, 1, precision=lax.Precision.HIGHEST)
    packed = packed - jnp.array([1.0, 1.0, 0.0, 0.0], f32)[:, None]
    packed = packed.reshape(2 * top_count, groups, group_rows).transpose(1, 0, 2)
    packed = jnp.pad(
        packed,
        ((0, 0), (0, 0), (0, LANES - group_rows)),
        constant_values=-1.0,
    )
    extra = jnp.broadcast_to(z_slot.astype(f32)[None, None, :], (groups, META_ROWS - 4, tok_rows))
    meta = jnp.concatenate([packed, extra], axis=1)

    token_in, cot_in, gate_in, meta_in = dispatch(
        tok_send.reshape(groups, group_rows, features),
        meta,
        moe_out,
        out_grad,
        norm_gain[None, :],
        plane_size,
        slots,
        t_count,
    )
    weight = gate_in[:, :z_count].astype(f32).T.reshape(-1)[:, None]
    row_block = token_in.reshape(devices * slots, features)
    cot_in = cot_in.reshape(devices * slots, features)
    w_gate_one = w_gate[0]
    w_up_one = w_up[0]
    w_down_one = w_down[0]
    pre_gate = jnp.dot(row_block, w_gate_one, preferred_element_type=f32)
    pre_up = jnp.dot(row_block, w_up_one, preferred_element_type=f32)
    sigmoid_gate = jax.nn.sigmoid(pre_gate)
    activated = pre_gate * sigmoid_gate
    hidden = activated * pre_up
    hid_grad = contract(cot_in, w_down_one, 1, 1)
    gate_grad = jnp.sum(hidden * hid_grad, axis=1).astype(bf16)
    d_hidden = weight * hid_grad
    d_gate = (d_hidden * pre_up * sigmoid_gate * (1.0 + pre_gate * (1.0 - sigmoid_gate))).astype(bf16)
    d_up = (d_hidden * activated).astype(bf16)
    token_back = (contract(d_gate, w_gate_one, 1, 1) + contract(d_up, w_up_one, 1, 1)).astype(bf16)
    scaled_cot = (weight * cot_in.astype(f32)).astype(bf16)
    grad_gate = contract(row_block, d_gate, 0, 0).astype(bf16)
    grad_up = contract(row_block, d_up, 0, 0).astype(bf16)
    grad_down = contract(hidden.astype(bf16), scaled_cot, 0, 0).astype(bf16)

    gg = jnp.pad(gate_grad.reshape(z_count, rows).T, ((0, 0), (0, LANES - z_count)))
    back, gback = combine(
        token_back.reshape(z_count, rows, features), gg, meta_in, group_rows, plane_size, slots
    )
    token_grad = contract(hit.astype(bf16), back.reshape(groups * group_rows, features), 0, 0).astype(bf16)
    gvals = gback[:, :top_count, :group_rows].transpose(1, 0, 2).reshape(top_count, groups * group_rows)
    gates_grad = jnp.sum(jnp.where(hit.T[:, None, :], gvals[None], 0.0), axis=2).astype(bf16)
    return (token_grad, gates_grad, grad_gate[None], grad_up[None], grad_down[None])


def solution(mesh):
    ep, tp = mesh.shape["ep"], mesh.shape["tp"]
    cut = Mesh(mesh.devices.reshape(groups, ep // groups, tp), AXES)
    rows, ep_axes = P(AXES, None), ("z", "x")
    cube = P(AXES, None, None)
    return jax.shard_map(
        local,
        mesh=cut,
        in_specs=(rows, rows, rows, cube, cube, cube, P(ep_axes, "tp"), P("tp"), P(ep_axes, "tp")),
        out_specs=(rows, rows, cube, cube, cube),
        check_vma=False,
    )
```

```python
import functools

import jax
import jax.numpy as jnp
from jax import lax
from jax.experimental import pallas as pl
from jax.experimental.pallas import tpu as pltpu
from jax.sharding import Mesh
from jax.sharding import PartitionSpec as P

epsilon = 1e-06
groups = 4
MESH = pl.DeviceIdType.MESH
AXES = ("z", "x", "tp")
META_ROWS = 8
LANES = 128


def contract(left, right, left_dim, right_dim, **kw):
    return lax.dot_general(
        left, right, (((left_dim,), (right_dim,)), ((), ())), preferred_element_type=jnp.float32, **kw
    )


def earlier_equal(ids):
    count = ids.shape[-1]
    place = jnp.arange(count, dtype=jnp.int32)
    same = (ids[..., :, None] == ids[..., None, :]) & (place[:, None] > place[None, :])
    return jnp.sum(same.astype(jnp.int32), axis=-1)


class Place:
    def __init__(self, plane_size):
        self.z, self.x, self.t = (lax.axis_index(name) for name in AXES)
        self.zc, self.tc = lax.axis_size("z"), lax.axis_size("tp")
        self.plane = plane_size
        self.own = self.x * self.tc + self.t

    def at(self, d, k=0):
        return (lax.rem(self.z + d, self.zc), self.x, lax.rem(self.t + k, self.tc))

    def back(self, d):
        return (lax.rem(self.z + self.zc - d, self.zc), self.x, self.t)

    def peer(self, k):
        q = lax.rem(self.own + k, self.plane)
        return q, (self.z, q // self.tc, lax.rem(q, self.tc))


def enter(place, wide):
    wait = greet_all(place, wide)
    wait()


def greet_all(place, wide):
    barrier = pltpu.get_barrier_semaphore()

    def greet(device):
        pl.semaphore_signal(barrier, inc=1, device_id=device, device_id_type=MESH)

    lax.fori_loop(1, place.plane, lambda k, c: (greet(place.peer(k)[1]), c)[1], 0)
    across = place.tc if wide else 1
    for d in range(1, place.zc):
        lax.fori_loop(0, across, lambda k, c: (greet(place.at(d, k)), c)[1], 0)
    return lambda: pl.semaphore_wait(barrier, place.plane - 1 + (place.zc - 1) * across)


def each(first, last, act):
    lax.fori_loop(first, last, lambda k, c: (act(k), c)[1], 0)


def columns(features, act):
    chunk = min(512, features)
    each(0, features // chunk, lambda c: act(pl.ds(pl.multiple_of(c * chunk, chunk), chunk)))


def iota(shape, dim):
    return lax.broadcasted_iota(jnp.int32, shape, dim)


def chosen(meta, row, slots, width):
    ids = meta[row : row + 1, :width].astype(jnp.int32)
    return iota((slots, width), 0) == ids


def picker(meta, slots, width):
    return (chosen(meta, 0, slots, width) | chosen(meta, 1, slots, width)).astype(
        jnp.float32
    ).astype(jnp.bfloat16)


def dispatch_kernel(
    plane_size, slots, tok_ref, meta_ref, saved_ref, grad_ref, gain_ref,
    tok_out, cot_out, w_out, meta_out,
    mbuf, stat, stbuf, cotz, ztok, zcot, stok, scot, wsend, wrecv,
    ms_sem, mr_sem, ss_sem, sr_sem, zs_sem, zr_sem, ps_sem, pr_sem, loc_sem, ws_sem, wr_sem,
):
    place = Place(plane_size)
    z, x, t, zc, tc = place.z, place.x, place.t, place.zc, place.tc
    own, peer = place.own, place.peer
    features = tok_ref.shape[-1]
    group_rows = tok_ref.shape[1]
    part = saved_ref.shape[-1]
    block = saved_ref.shape[0] // tc
    all_slots = plane_size * slots
    bf16 = jnp.bfloat16
    enter(place, True)

    def rows_of(q):
        return pl.ds(pl.multiple_of(q * slots, slots), slots)

    def remote(src, dst, send, recv, device):
        return pltpu.make_async_remote_copy(
            src_ref=src, dst_ref=dst, send_sem=send, recv_sem=recv, device_id=device, device_id_type=MESH
        )

    def meta_copy(d, k):
        return remote(
            meta_ref.at[lax.rem(z + d, zc)], mbuf.at[d, t], ms_sem.at[d, k], mr_sem.at[d, k], place.at(d, k)
        )

    def stat_copy(k):
        return remote(stat, stbuf.at[k], ss_sem.at[k], sr_sem.at[k], place.at(0, k))

    def z_copy(a, d):
        src, dst = ((tok_ref, ztok), (cotz, zcot))[a]
        return remote(
            src.at[lax.rem(z + d, zc)], dst.at[d], zs_sem.at[a, d], zr_sem.at[a, d], place.at(d)
        )

    def plane_parts(a, d, q):
        if a == 0:
            return stok.at[d, rows_of(q)], tok_out.at[d, rows_of(own)]
        cols = pl.ds(pl.multiple_of(t * part, part), part)
        return scot.at[d, :, rows_of(q)], cot_out.at[d, x, :, :, cols]

    def plane_copy(a, d, k):
        q, device = peer(k)
        src, dst = plane_parts(a, d, q)
        return remote(src, dst, ps_sem.at[a, d, k], pr_sem.at[a, d, k], device)

    def own_copy(a, d):
        src, dst = plane_parts(a, d, own)
        return pltpu.make_async_copy(src, dst, loc_sem.at[a, d])

    def w_copy(k):
        q, device = peer(k)
        return remote(wsend.at[rows_of(q)], wrecv.at[rows_of(own)], ws_sem.at[k], wr_sem.at[k], device)

    def spread_out(a, d):
        each(1, plane_size, lambda k: plane_copy(a, d, k).start())
        own_copy(a, d).start()

    def send_tok(d):
        sel = picker(mbuf[d, t], all_slots, group_rows)

        def one(cols):
            rows = ztok[d, :, cols] if d else tok_ref[z, :, cols]
            stok[d, :, cols] = jnp.dot(sel, rows, preferred_element_type=jnp.float32).astype(bf16)

        columns(features, one)
        spread_out(0, d)

    def send_cot(d):
        for b in range(tc):
            sel = picker(mbuf[d, b], all_slots, group_rows)
            rows = slice(b * group_rows, (b + 1) * group_rows)
            value = zcot[d, rows, :] if d else cotz[z, rows, :]
            scot[d, b] = jnp.dot(sel, value, preferred_element_type=jnp.float32).astype(bf16)
        spread_out(1, d)

    mbuf[0, t] = meta_ref[z]
    for d in range(zc):
        each(0 if d else 1, tc, lambda k: meta_copy(d, k).start())
    for d in range(1, zc):
        z_copy(0, d).start()

    eye = iota((block, block), 0) == iota((block, block), 1)
    gain = gain_ref[...]
    for b in range(tc):
        rows = slice(b * block, (b + 1) * block)
        saved = saved_ref[rows, :].astype(jnp.float32)
        scaled = gain * grad_ref[rows, :].astype(jnp.float32)
        for i, value in enumerate((saved * saved, saved * scaled)):
            total = jnp.sum(value, axis=1, keepdims=True)
            row = i * tc + b
            stat[row : row + 1, :] = jnp.sum(jnp.where(eye, total, 0.0), axis=0, keepdims=True)
    each(1, tc, lambda k: stat_copy(k).start())

    send_tok(0)

    each(1, tc, lambda k: stat_copy(k).wait_recv())
    each(1, tc, lambda k: meta_copy(0, k).wait_recv())
    totals = stat[...]
    for k in range(1, tc):
        totals = totals + stbuf[k]
    inv = lax.rsqrt(totals[:tc] / features + epsilon)
    coef = inv * inv * inv * totals[tc:] / features
    for b in range(tc):
        rows = slice(b * block, (b + 1) * block)
        saved = saved_ref[rows, :].astype(jnp.float32)
        scaled = gain * grad_ref[rows, :].astype(jnp.float32)
        inv_col = jnp.sum(jnp.where(eye, inv[b : b + 1], 0.0), axis=1, keepdims=True)
        coef_col = jnp.sum(jnp.where(eye, coef[b : b + 1], 0.0), axis=1, keepdims=True)
        cot = (inv_col * scaled - saved * coef_col).astype(bf16)
        pack = chosen(mbuf[0, b], 4, zc * group_rows, block).astype(jnp.float32).astype(bf16)
        packed = jnp.dot(pack, cot, preferred_element_type=jnp.float32).astype(bf16)
        for g in range(zc):
            cotz[g, b * group_rows : (b + 1) * group_rows, :] = packed[g * group_rows : (g + 1) * group_rows]
    for d in range(1, zc):
        z_copy(1, d).start()
    send_cot(0)

    for d in range(1, zc):
        each(0, tc, lambda k: meta_copy(d, k).wait_recv())
    weights = jnp.zeros((all_slots, LANES), jnp.float32)
    for d in range(zc):
        meta = mbuf[d, t]
        meta_out[d] = meta
        total = jnp.zeros((all_slots, 1), jnp.float32)
        for i in range(2):
            hit = chosen(meta, i, all_slots, group_rows)
            total = total + jnp.sum(
                jnp.where(hit, meta[2 + i : 3 + i, :group_rows], 0.0), axis=1, keepdims=True
            )
        weights = jnp.where(iota((all_slots, LANES), 1) == d, total, weights)
    wsend[...] = weights.astype(bf16)
    each(1, plane_size, lambda k: w_copy(k).start())
    wrecv[rows_of(own)] = wsend[rows_of(own)]

    for d in range(1, zc):
        z_copy(0, d).wait_recv()
        send_tok(d)
    for d in range(1, zc):
        z_copy(1, d).wait_recv()
        send_cot(d)

    each(1, plane_size, lambda k: w_copy(k).wait_recv())
    w_out[...] = wrecv[...]
    for a in range(2):
        for d in range(zc):
            own_copy(a, d).wait()
            each(1, plane_size, lambda k: plane_copy(a, d, k).wait(), )
            if d:
                z_copy(a, d).wait_send()
    for d in range(zc):
        each(0 if d else 1, tc, lambda k: meta_copy(d, k).wait_send())
    each(1, tc, lambda k: stat_copy(k).wait_send())
    each(1, plane_size, lambda k: w_copy(k).wait_send())


def combine_kernel(
    plane_size, slots, back_ref, gg_ref, meta_ref, out_ref, gout_ref,
    rbuf, cbuf, ggbuf, gbuf, gland, zs_sem, zr_sem, ps_sem, pr_sem, loc_sem, own_sem,
    gs_sem, gr_sem, gzs_sem, gzr_sem,
):
    place = Place(plane_size)
    z, zc, own, peer = place.z, place.zc, place.own, place.peer
    features = back_ref.shape[-1]
    group_rows = out_ref.shape[1]
    all_slots = plane_size * slots
    enter(place, False)

    def rows_of(q):
        return pl.ds(pl.multiple_of(q * slots, slots), slots)

    def remote(src, dst, send, recv, device):
        return pltpu.make_async_remote_copy(
            src_ref=src, dst_ref=dst, send_sem=send, recv_sem=recv, device_id=device, device_id_type=MESH
        )

    def plane_copy(d, k):
        q, device = peer(k)
        return remote(
            back_ref.at[d, rows_of(q)], rbuf.at[d, rows_of(own)], ps_sem.at[d, k], pr_sem.at[d, k], device
        )

    def own_rows(d):
        return pltpu.make_async_copy(back_ref.at[d, rows_of(own)], rbuf.at[d, rows_of(own)], loc_sem.at[d])

    def gg_copy(k):
        q, device = peer(k)
        return remote(gg_ref.at[rows_of(q)], ggbuf.at[rows_of(own)], gs_sem.at[k], gr_sem.at[k], device)

    def z_copy(d):
        return remote(cbuf.at[d], out_ref.at[z], zs_sem.at[d], zr_sem.at[d], place.back(d))

    def gz_copy(d):
        return remote(gbuf.at[d], gland.at[z], gzs_sem.at[d], gzr_sem.at[d], place.back(d))

    keep = pltpu.make_async_copy(cbuf.at[0], out_ref.at[z], own_sem)
    order = list(range(1, zc)) + [0]
    each(1, plane_size, lambda k: gg_copy(k).start())
    ggbuf[rows_of(own)] = gg_ref[rows_of(own)]
    for d in order:
        own_rows(d).start()
        each(1, plane_size, lambda k: plane_copy(d, k).start())
    each(1, plane_size, lambda k: gg_copy(k).wait_recv())
    returned = ggbuf[...].astype(jnp.float32)
    for d in order:
        meta = meta_ref[d]
        column = jnp.sum(
            jnp.where(iota(returned.shape, 1) == d, returned, 0.0), axis=1, keepdims=True
        )
        for i in range(2):
            hit = chosen(meta, i, all_slots, LANES)
            gbuf[d, i : i + 1, :] = jnp.sum(jnp.where(hit, column, 0.0), axis=0, keepdims=True)
        if d:
            gz_copy(d).start()
        else:
            gland[z] = gbuf[0]
    for d in order:
        own_rows(d).wait()
        each(1, plane_size, lambda k: plane_copy(d, k).wait_recv())
        sel = picker(meta_ref[d], all_slots, group_rows)

        def one(cols):
            cbuf[d, :, cols] = contract(sel, rbuf[d, :, cols], 0, 0).astype(cbuf.dtype)

        columns(features, one)
        if d:
            z_copy(d).start()
        else:
            keep.start()
    for d in order:
        each(1, plane_size, lambda k: plane_copy(d, k).wait_send())
        if d:
            gz_copy(d).wait()
            z_copy(d).wait()
    keep.wait()
    gout_ref[...] = gland[...]
    each(1, plane_size, lambda k: gg_copy(k).wait_send())


def vmem():
    return pl.BlockSpec(memory_space=pltpu.VMEM)


def anywhere():
    return pl.BlockSpec(memory_space=pl.ANY)


def dispatch(tok_send, meta, saved, grad, gain, plane_size, slots, tc):
    zc, group_rows, features = tok_send.shape
    part = saved.shape[1]
    rows = plane_size * slots
    bf16 = tok_send.dtype
    dma, struct, space = pltpu.SemaphoreType.DMA, jax.ShapeDtypeStruct, pltpu.VMEM
    f32 = jnp.float32
    return pl.pallas_call(
        functools.partial(dispatch_kernel, plane_size, slots),
        out_shape=(
            struct((zc, rows, features), bf16),
            struct((zc, plane_size // tc, tc, slots, features), bf16),
            struct((rows, LANES), bf16),
            struct(meta.shape, f32),
        ),
        in_specs=[vmem()] * 5,
        out_specs=(anywhere(), anywhere(), vmem(), vmem()),
        scratch_shapes=[
            space((zc, tc, META_ROWS, LANES), f32),
            space((2 * tc, LANES), f32),
            space((tc, 2 * tc, LANES), f32),
            space((zc, tc * group_rows, part), bf16),
            space((zc, group_rows, features), bf16),
            space((zc, tc * group_rows, part), bf16),
            space((zc, rows, features), bf16),
            space((zc, tc, rows, part), bf16),
            space((rows, LANES), bf16),
            space((rows, LANES), bf16),
            dma((zc, tc)),
            dma((zc, tc)),
            dma((tc,)),
            dma((tc,)),
            dma((2, zc)),
            dma((2, zc)),
            dma((2, zc, plane_size)),
            dma((2, zc, plane_size)),
            dma((2, zc)),
            dma((plane_size,)),
            dma((plane_size,)),
        ],
        compiler_params=pltpu.CompilerParams(
            collective_id=0, has_side_effects=True, vmem_limit_bytes=48 * 1024 * 1024
        ),
        name="dispatch",
    )(tok_send, meta, saved, grad, gain)


def combine(back, gg, meta, group_rows, plane_size, slots):
    zc, rows, features = back.shape
    dma, struct, space = pltpu.SemaphoreType.DMA, jax.ShapeDtypeStruct, pltpu.VMEM
    return pl.pallas_call(
        functools.partial(combine_kernel, plane_size, slots),
        out_shape=(struct((zc, group_rows, features), back.dtype), struct(meta.shape, meta.dtype)),
        in_specs=[anywhere(), vmem(), vmem()],
        out_specs=(anywhere(), vmem()),
        scratch_shapes=[
            space(back.shape, back.dtype),
            space((zc, group_rows, features), back.dtype),
            space(gg.shape, gg.dtype),
            space(meta.shape, meta.dtype),
            space(meta.shape, meta.dtype),
            dma((zc,)),
            dma((zc,)),
            dma((zc, plane_size)),
            dma((zc, plane_size)),
            dma((zc,)),
            dma(()),
            dma((plane_size,)),
            dma((plane_size,)),
            dma((zc,)),
            dma((zc,)),
        ],
        compiler_params=pltpu.CompilerParams(
            collective_id=1, has_side_effects=True, vmem_limit_bytes=48 * 1024 * 1024
        ),
        name="combine",
    )(back, gg, meta)


def apart(tokens, routes, gates, w_gate, w_up, w_down, moe_out, norm_gain, out_grad):
    z_count, x_count, t_count = (lax.axis_size(name) for name in AXES)
    plane_size = x_count * t_count
    devices = z_count * plane_size
    tok_rows, features = tokens.shape
    top_count = routes.shape[1]
    capacity = groups * tok_rows // devices
    slots = -(-capacity // 16) * 16
    group_rows = 3 * tok_rows // 8
    rows = plane_size * slots
    bf16, f32 = jnp.bfloat16, jnp.float32

    own_ids = routes.T.reshape(-1)
    own_group = routes[:, 0] // plane_size
    z_slot = own_group * group_rows + earlier_equal(own_group)
    hit = jnp.arange(groups * group_rows, dtype=jnp.int32)[:, None] == z_slot[None, :]
    tok_send = jnp.dot(hit.astype(bf16), tokens, preferred_element_type=f32).astype(bf16)
    slot_of = (own_ids % plane_size) * slots + earlier_equal(own_ids)
    values = jnp.concatenate(
        [
            slot_of.reshape(top_count, tok_rows).astype(f32) + 1.0,
            gates.T.astype(bf16).astype(f32),
        ]
    )
    packed = contract(values, hit.astype(f32), 1, 1, precision=lax.Precision.HIGHEST)
    packed = packed - jnp.array([1.0, 1.0, 0.0, 0.0], f32)[:, None]
    packed = packed.reshape(2 * top_count, groups, group_rows).transpose(1, 0, 2)
    packed = jnp.pad(
        packed,
        ((0, 0), (0, 0), (0, LANES - group_rows)),
        constant_values=-1.0,
    )
    extra = jnp.broadcast_to(z_slot.astype(f32)[None, None, :], (groups, META_ROWS - 4, tok_rows))
    meta = jnp.concatenate([packed, extra], axis=1)

    token_in, cot_in, gate_in, meta_in = dispatch(
        tok_send.reshape(groups, group_rows, features),
        meta,
        moe_out,
        out_grad,
        norm_gain[None, :],
        plane_size,
        slots,
        t_count,
    )
    weight = gate_in[:, :z_count].astype(f32).T.reshape(-1)[:, None]
    row_block = token_in.reshape(devices * slots, features)
    cot_in = cot_in.reshape(devices * slots, features)
    w_gate_one = w_gate[0]
    w_up_one = w_up[0]
    w_down_one = w_down[0]
    pre_gate = jnp.dot(row_block, w_gate_one, preferred_element_type=f32)
    pre_up = jnp.dot(row_block, w_up_one, preferred_element_type=f32)
    sigmoid_gate = jax.nn.sigmoid(pre_gate)
    activated = pre_gate * sigmoid_gate
    hidden = activated * pre_up
    hid_grad = contract(cot_in, w_down_one, 1, 1)
    gate_grad = jnp.sum(hidden * hid_grad, axis=1).astype(bf16)
    d_hidden = weight * hid_grad
    d_gate = (d_hidden * pre_up * sigmoid_gate * (1.0 + pre_gate * (1.0 - sigmoid_gate))).astype(bf16)
    d_up = (d_hidden * activated).astype(bf16)
    token_back = (contract(d_gate, w_gate_one, 1, 1) + contract(d_up, w_up_one, 1, 1)).astype(bf16)
    scaled_cot = (weight * cot_in.astype(f32)).astype(bf16)
    grad_gate = contract(row_block, d_gate, 0, 0).astype(bf16)
    grad_up = contract(row_block, d_up, 0, 0).astype(bf16)
    grad_down = contract(hidden.astype(bf16), scaled_cot, 0, 0).astype(bf16)

    gg = jnp.pad(gate_grad.reshape(z_count, rows).T, ((0, 0), (0, LANES - z_count)))
    back, gback = combine(
        token_back.reshape(z_count, rows, features), gg, meta_in, group_rows, plane_size, slots
    )
    token_grad = contract(hit.astype(bf16), back.reshape(groups * group_rows, features), 0, 0).astype(bf16)
    gvals = gback[:, :top_count, :group_rows].transpose(1, 0, 2).reshape(top_count, groups * group_rows)
    gates_grad = jnp.sum(jnp.where(hit.T[:, None, :], gvals[None], 0.0), axis=2).astype(bf16)
    return (token_grad, gates_grad, grad_gate[None], grad_up[None], grad_down[None])


def fused_kernel(
    plane_size, slots, tok_hbm, route_hbm, gate_hbm, saved_hbm, grad_hbm, gain_hbm, wg_hbm, wu_hbm, wd_hbm,
    tg_ref, gg_out, dwg_ref, dwu_ref, dwd_ref,
    route_ref, gate_ref, gain_ref, tok, saved_ref, grad_ref, wg, wu, wd, meta, mbuf, stat, stbuf, tokz, cotz, ztok, zcot, stok, scot,
    wsend, wrecv, tok_in, cot_in, hid, dg, du, back, rbuf, cbuf, land, ggsend, ggbuf, gbuf, gland,
    in_sem, ms_sem, mr_sem, ss_sem, sr_sem, zs_sem, zr_sem, ps_sem, pr_sem, ws_sem, wr_sem,
    rs_sem, rr_sem, os_sem, or_sem, gs_sem, gr_sem, gzs_sem, gzr_sem,
):
    place = Place(plane_size)
    z, x, t, zc, tc = place.z, place.x, place.t, place.zc, place.tc
    own, peer = place.own, place.peer
    block, features = tok.shape
    part = saved_ref.shape[-1]
    group_rows = tokz.shape[1]
    chunk = plane_size * slots
    width = wg.shape[-1]
    bf16, f32 = jnp.bfloat16, jnp.float32

    loads = [
        pltpu.make_async_copy(src, dst, in_sem.at[i])
        for i, (src, dst) in enumerate(
            (
                (route_hbm, route_ref),
                (gate_hbm, gate_ref),
                (tok_hbm, tok),
                (gain_hbm, gain_ref),
                (saved_hbm, saved_ref),
                (grad_hbm, grad_ref),
                (wg_hbm.at[0], wg),
                (wu_hbm.at[0], wu),
                (wd_hbm.at[0], wd),
            )
        )
    ]
    for load in loads[:6]:
        load.start()
    everyone = greet_all(place, True)

    def rows_of(q):
        return pl.ds(pl.multiple_of(q * slots, slots), slots)

    def chunk_rows(d, q):
        return pl.ds(pl.multiple_of(d * chunk + q * slots, slots), slots)

    def remote(src, dst, send, recv, device):
        return pltpu.make_async_remote_copy(
            src_ref=src, dst_ref=dst, send_sem=send, recv_sem=recv, device_id=device, device_id_type=MESH
        )

    def meta_copy(d, k):
        return remote(
            meta.at[lax.rem(z + d, zc)], mbuf.at[d, t], ms_sem.at[d, k], mr_sem.at[d, k], place.at(d, k)
        )

    def stat_copy(k):
        return remote(stat, stbuf.at[k], ss_sem.at[k], sr_sem.at[k], place.at(0, k))

    def z_copy(a, d):
        src, dst = ((tokz, ztok), (cotz, zcot))[a]
        return remote(
            src.at[lax.rem(z + d, zc)], dst.at[d], zs_sem.at[a, d], zr_sem.at[a, d], place.at(d)
        )

    def plane_parts(a, d, q):
        if a == 0:
            return stok.at[d, rows_of(q)], tok_in.at[chunk_rows(d, own)]
        cols = pl.ds(pl.multiple_of(t * part, part), part)
        span = tc * slots
        rows = pl.ds(pl.multiple_of(d * chunk + x * span, span), span)
        return scot.at[d, q], cot_in.at[rows, cols]

    def plane_copy(a, d, k):
        q, device = peer(k)
        src, dst = plane_parts(a, d, q)
        return remote(src, dst, ps_sem.at[a, d, k], pr_sem.at[a, d, k], device)

    def w_copy(k):
        q, device = peer(k)
        return remote(wsend.at[rows_of(q)], wrecv.at[rows_of(own)], ws_sem.at[k], wr_sem.at[k], device)

    def return_copy(d, k):
        q, device = peer(k)
        return remote(
            back.at[d, rows_of(q)], rbuf.at[d, rows_of(own)], rs_sem.at[d, k], rr_sem.at[d, k], device
        )

    def out_copy(d):
        return remote(cbuf.at[d], land.at[z], os_sem.at[d], or_sem.at[d], place.back(d))

    def gg_copy(k):
        q, device = peer(k)
        return remote(ggsend.at[rows_of(q)], ggbuf.at[rows_of(own)], gs_sem.at[k], gr_sem.at[k], device)

    def gz_copy(d):
        return remote(gbuf.at[d], gland.at[z], gzs_sem.at[d], gzr_sem.at[d], place.back(d))

    def to_peers(copy):
        each(1, plane_size, lambda k: copy(k).start())

    def send_tok(d):
        sel = picker(mbuf[d, t], chunk, group_rows)

        def one(cols):
            rows = ztok[d, :, cols] if d else tokz[z, :, cols]
            stok[d, :, cols] = jnp.dot(sel, rows, preferred_element_type=f32).astype(bf16)

        columns(features, one)
        to_peers(lambda k: plane_copy(0, d, k))
        tok_in[chunk_rows(d, own), :] = stok[d, rows_of(own), :]

    def send_cot(d):
        for b in range(tc):
            sel = picker(mbuf[d, b], chunk, group_rows)
            rows = slice(b * group_rows, (b + 1) * group_rows)
            value = zcot[d, rows, :] if d else cotz[z, rows, :]
            value = jnp.dot(sel, value, preferred_element_type=f32).astype(bf16)
            for q in range(plane_size):
                scot[d, q, b * slots : (b + 1) * slots, :] = value[q * slots : (q + 1) * slots]
        to_peers(lambda k: plane_copy(1, d, k))
        src, dst = plane_parts(1, d, own)
        dst[...] = src[...]

    eye = iota((block, block), 0) == iota((block, block), 1)
    before = iota((block, block), 0) < iota((block, block), 1)

    def column(row):
        return jnp.sum(jnp.where(eye, row, 0.0), axis=1, keepdims=True)

    def count(mask):
        return jnp.sum(mask.astype(f32), axis=0, keepdims=True)

    loads[0].wait()
    loads[1].wait()
    ids = route_ref[...].astype(f32)
    ids = [ids[i : i + 1] for i in range(2)]
    id_cols = [column(row) for row in ids]
    group = sum((ids[0] >= float(g * plane_size)).astype(f32) for g in range(1, zc))
    z_slot = group * group_rows + count((column(group) == group) & before)
    ranks = [
        count((id_cols[0] == ids[0]) & before),
        count(id_cols[0] == ids[1]) + count((id_cols[1] == ids[1]) & before),
    ]
    values = [(ids[i] - group * plane_size) * slots + ranks[i] + 1.0 for i in range(2)]
    values += [gate_ref[i : i + 1].astype(bf16).astype(f32) for i in range(2)]
    value_cols = [column(row) for row in values]
    slot_col = column(z_slot)
    lane = iota((block, block), 1).astype(f32)
    for g in range(zc):
        hit = (slot_col == lane + float(g * group_rows)) & (lane < float(group_rows))
        for i in range(4):
            row = jnp.sum(jnp.where(hit, value_cols[i], 0.0), axis=0, keepdims=True)
            meta[g, i : i + 1, :] = row - 1.0 if i < 2 else row
        meta[g, 4:8, :] = jnp.broadcast_to(z_slot, (4, block))

    def packer(row):
        slot = iota((zc * group_rows, block), 0).astype(f32)
        return (slot == row).astype(f32).astype(bf16)

    own_pack = packer(z_slot)
    loads[2].wait()

    def pack_tokens(cols):
        value = jnp.dot(own_pack, tok[:, cols], preferred_element_type=f32).astype(bf16)
        for g in range(zc):
            tokz[g, :, cols] = value[g * group_rows : (g + 1) * group_rows]

    columns(features, pack_tokens)
    everyone()

    for d in range(zc):
        each(0 if d else 1, tc, lambda k: meta_copy(d, k).start())
    for d in range(1, zc):
        z_copy(0, d).start()
    mbuf[0, t] = meta[z]

    for load in loads[6:]:
        load.start()
    for load in loads[3:6]:
        load.wait()
    gain = gain_ref[...]
    for b in range(tc):
        rows = slice(b * block, (b + 1) * block)
        saved = saved_ref[rows, :].astype(f32)
        scaled = gain * grad_ref[rows, :].astype(f32)
        for i, value in enumerate((saved * saved, saved * scaled)):
            total = jnp.sum(value, axis=1, keepdims=True)
            row = i * tc + b
            stat[row : row + 1, :] = jnp.sum(jnp.where(eye, total, 0.0), axis=0, keepdims=True)
    each(1, tc, lambda k: stat_copy(k).start())

    send_tok(0)

    each(1, tc, lambda k: stat_copy(k).wait_recv())
    each(1, tc, lambda k: meta_copy(0, k).wait_recv())
    totals = stat[...]
    for k in range(1, tc):
        totals = totals + stbuf[k]
    inv = lax.rsqrt(totals[:tc] / features + epsilon)
    coef = inv * inv * inv * totals[tc:] / features
    for b in range(tc):
        rows = slice(b * block, (b + 1) * block)
        saved = saved_ref[rows, :].astype(f32)
        scaled = gain * grad_ref[rows, :].astype(f32)
        cot = (column(inv[b : b + 1]) * scaled - saved * column(coef[b : b + 1])).astype(bf16)
        packed = jnp.dot(packer(mbuf[0, b, 4:5, :]), cot, preferred_element_type=f32).astype(bf16)
        for g in range(zc):
            cotz[g, b * group_rows : (b + 1) * group_rows, :] = packed[g * group_rows : (g + 1) * group_rows]
    for d in range(1, zc):
        z_copy(1, d).start()
    send_cot(0)

    for d in range(1, zc):
        each(0, tc, lambda k: meta_copy(d, k).wait_recv())
    weights = jnp.zeros((chunk, LANES), f32)
    for d in range(zc):
        tile = mbuf[d, t]
        total = jnp.zeros((chunk, 1), f32)
        for i in range(2):
            hit = chosen(tile, i, chunk, group_rows)
            total = total + jnp.sum(
                jnp.where(hit, tile[2 + i : 3 + i, :group_rows], 0.0), axis=1, keepdims=True
            )
        weights = jnp.where(iota((chunk, LANES), 1) == d, total, weights)
    wsend[...] = weights.astype(bf16)
    to_peers(w_copy)
    wrecv[rows_of(own)] = wsend[rows_of(own)]

    def weight_of(d):
        tile = wrecv[...].astype(f32)
        return jnp.sum(jnp.where(iota(tile.shape, 1) == d, tile, 0.0), axis=1, keepdims=True)

    def compute(d):
        rows = slice(d * chunk, (d + 1) * chunk)
        for a in range(2):
            each(1, plane_size, lambda k: plane_copy(a, d, k).wait_recv())
        weight = weight_of(d)
        step = 256

        def forward(c, total):
            cols = pl.ds(pl.multiple_of(c * step, step), step)
            token = tok_in[rows, :]
            pre_gate = jnp.dot(token, wg[:, cols], preferred_element_type=f32)
            pre_up = jnp.dot(token, wu[:, cols], preferred_element_type=f32)
            hid_grad = contract(cot_in[rows, :], wd[cols, :], 1, 1)
            sigmoid = jax.nn.sigmoid(pre_gate)
            activated = pre_gate * sigmoid
            hidden = activated * pre_up
            d_hidden = weight * hid_grad
            hid[rows, cols] = hidden.astype(bf16)
            dg[rows, cols] = (d_hidden * pre_up * sigmoid * (1.0 + pre_gate * (1.0 - sigmoid))).astype(bf16)
            du[rows, cols] = (d_hidden * activated).astype(bf16)
            return total + jnp.sum(hidden * hid_grad, axis=1, keepdims=True)

        total = lax.fori_loop(0, width // step, forward, jnp.zeros((chunk, 1), f32))

        def backward(cols):
            value = contract(dg[rows, :], wg[cols, :], 1, 1) + contract(du[rows, :], wu[cols, :], 1, 1)
            back[d, :, cols] = value.astype(bf16)
            cot_in[rows, cols] = (weight * cot_in[rows, cols].astype(f32)).astype(bf16)

        columns(features, backward)
        return total

    def give_back(d):
        to_peers(lambda k: return_copy(d, k))
        rbuf[d, rows_of(own)] = back[d, rows_of(own)]

    def unite(d):
        each(1, plane_size, lambda k: return_copy(d, k).wait_recv())
        sel = picker(mbuf[d, t], chunk, group_rows)

        def one(cols):
            value = contract(sel, rbuf[d, :, cols], 0, 0).astype(bf16)
            if d:
                cbuf[d, :, cols] = value
            else:
                land[z, :, cols] = value

        columns(features, one)
        if d:
            out_copy(d).start()

    def weight_grad(out, left, right):
        step = min(256, out.shape[0])

        def one(c):
            cols = pl.ds(pl.multiple_of(c * step, step), step)
            out[cols, :] = contract(left[:, cols], right[...], 0, 0).astype(bf16)

        each(0, out.shape[0] // step, one)

    sums = [None] * zc
    for d in range(1, zc):
        z_copy(0, d).wait_recv()
        send_tok(d)
        if d == 1:
            for load in loads[6:]:
                load.wait()
            each(1, plane_size, lambda k: w_copy(k).wait_recv())
            sums[0] = compute(0)
    for d in range(1, zc):
        z_copy(1, d).wait_recv()
        send_cot(d)
    for d in range(1, zc):
        sums[d] = compute(d)
        if d < zc - 1:
            give_back(d)
    tile = jnp.zeros((chunk, LANES), f32)
    for d in range(zc):
        tile = jnp.where(iota((chunk, LANES), 1) == d, sums[d], tile)
    ggsend[...] = tile.astype(bf16)
    to_peers(gg_copy)
    ggbuf[rows_of(own)] = ggsend[rows_of(own)]
    give_back(zc - 1)
    give_back(0)

    grads = [(dwg_ref, tok_in, dg), (dwu_ref, tok_in, du), (dwd_ref, hid, cot_in)]
    for d in range(1, zc):
        unite(d)
        if grads:
            weight_grad(*grads.pop(0))
    each(1, plane_size, lambda k: gg_copy(k).wait_recv())
    returned = ggbuf[...].astype(f32)
    for d in range(zc):
        picked = jnp.sum(jnp.where(iota(returned.shape, 1) == d, returned, 0.0), axis=1, keepdims=True)
        for i in range(2):
            hit = chosen(mbuf[d, t], i, chunk, LANES)
            gbuf[d, i : i + 1, :] = jnp.sum(jnp.where(hit, picked, 0.0), axis=0, keepdims=True)
        if d:
            gz_copy(d).start()
    gland[z] = gbuf[0]
    unite(0)

    for d in range(1, zc):
        gz_copy(d).wait_recv()
        out_copy(d).wait_recv()

    def unpack(cols):
        total = jnp.zeros((block, cols.size), f32)
        for g in range(zc):
            total = total + contract(own_pack[g * group_rows : (g + 1) * group_rows], land[g, :, cols], 0, 0)
        tg_ref[:, cols] = total.astype(bf16)

    columns(features, unpack)
    slot_col = column(mbuf[0, t, 4:5, :])
    slot_row = mbuf[0, t, 4:5, :]
    for i in range(2):
        row = jnp.zeros((1, block), f32)
        for g in range(zc):
            source = column(gland[g, i : i + 1, :])
            hit = iota((block, block), 0).astype(f32) + float(g * group_rows) == slot_row
            hit = hit & (iota((block, block), 0) < group_rows)
            row = row + jnp.sum(jnp.where(hit, source, 0.0), axis=0, keepdims=True)
        gg_out[i : i + 1, :] = row

    for d in range(zc):
        each(0 if d else 1, tc, lambda k: meta_copy(d, k).wait_send())
        for a in range(2):
            each(1, plane_size, lambda k: plane_copy(a, d, k).wait_send())
            if d:
                z_copy(a, d).wait_send()
        each(1, plane_size, lambda k: return_copy(d, k).wait_send())
        if d:
            out_copy(d).wait_send()
            gz_copy(d).wait_send()
    each(1, tc, lambda k: stat_copy(k).wait_send())
    each(1, plane_size, lambda k: w_copy(k).wait_send())
    each(1, plane_size, lambda k: gg_copy(k).wait_send())


def fused_scratch(block, features, part, width, group_rows, zc, tc, plane_size, slots):
    bf16, f32, space = jnp.bfloat16, jnp.float32, pltpu.VMEM
    rows = plane_size * slots
    tile = (META_ROWS, LANES)
    return [
        space((2, block), jnp.int32),
        space((2, block), f32),
        space((1, part), f32),
        space((block, features), bf16),
        space((tc * block, part), bf16),
        space((tc * block, part), bf16),
        space((features, width), bf16),
        space((features, width), bf16),
        space((width, features), bf16),
        space((zc,) + tile, f32),
        space((zc, tc) + tile, f32),
        space((2 * tc, LANES), f32),
        space((tc, 2 * tc, LANES), f32),
        space((zc, group_rows, features), bf16),
        space((zc, tc * group_rows, part), bf16),
        space((zc, group_rows, features), bf16),
        space((zc, tc * group_rows, part), bf16),
        space((zc, rows, features), bf16),
        space((zc, plane_size, tc * slots, part), bf16),
        space((rows, LANES), bf16),
        space((rows, LANES), bf16),
        space((zc * rows, features), bf16),
        space((zc * rows, features), bf16),
        space((zc * rows, width), bf16),
        space((zc * rows, width), bf16),
        space((zc * rows, width), bf16),
        space((zc, rows, features), bf16),
        space((zc, rows, features), bf16),
        space((zc, group_rows, features), bf16),
        space((zc, group_rows, features), bf16),
        space((rows, LANES), bf16),
        space((rows, LANES), bf16),
        space((zc,) + tile, f32),
        space((zc,) + tile, f32),
    ]


def fused(tokens, routes, gates, saved, grad, gain, w_gate, w_up, w_down, scratch, limit, plane_size, slots, zc, tc):
    dma, struct = pltpu.SemaphoreType.DMA, jax.ShapeDtypeStruct
    bf16, f32 = jnp.bfloat16, jnp.float32
    semaphores = [
        dma((9,)),
        dma((zc, tc)),
        dma((zc, tc)),
        dma((tc,)),
        dma((tc,)),
        dma((2, zc)),
        dma((2, zc)),
        dma((2, zc, plane_size)),
        dma((2, zc, plane_size)),
        dma((plane_size,)),
        dma((plane_size,)),
        dma((zc, plane_size)),
        dma((zc, plane_size)),
        dma((zc,)),
        dma((zc,)),
        dma((plane_size,)),
        dma((plane_size,)),
        dma((zc,)),
        dma((zc,)),
    ]
    operands = (tokens, routes, gates, saved, grad, gain, w_gate, w_up, w_down)
    space = pltpu.MemorySpace.HBM
    hbm = pl.BlockSpec(memory_space=space)
    return pl.pallas_call(
        functools.partial(fused_kernel, plane_size, slots),
        out_shape=(
            struct(tokens.shape, bf16),
            struct(routes.shape, f32),
            struct(w_gate.shape[1:], bf16),
            struct(w_up.shape[1:], bf16),
            struct(w_down.shape[1:], bf16),
        ),
        in_specs=[hbm] * 9,
        out_specs=(vmem(),) * 5,
        scratch_shapes=scratch + semaphores,
        compiler_params=pltpu.CompilerParams(
            collective_id=2, has_side_effects=True, vmem_limit_bytes=limit
        ),
        name="layer",
    )(*(pltpu.with_memory_space_constraint(value, space) for value in operands))


def size_of(refs):
    total = 0
    for ref in refs:
        count = ref.dtype.itemsize if hasattr(ref.dtype, "itemsize") else jnp.dtype(ref.dtype).itemsize
        for extent in ref.shape:
            count *= extent
        total += count
    return total


MIB = 1024 * 1024


def put_kernel(*refs):
    count = len(refs) // 2
    copies = [pltpu.make_async_copy(refs[i], refs[count + i], refs[-1].at[i]) for i in range(count)]
    for copy in copies:
        copy.start()
    for copy in copies:
        copy.wait()


def put_out(*values):
    return pl.pallas_call(
        put_kernel,
        out_shape=tuple(jax.ShapeDtypeStruct(value.shape, value.dtype) for value in values),
        in_specs=[vmem()] * len(values),
        out_specs=(anywhere(),) * len(values),
        scratch_shapes=[pltpu.SemaphoreType.DMA((len(values),))],
        compiler_params=pltpu.CompilerParams(vmem_limit_bytes=MIB),
        name="put",
    )(*values)


def local(tokens, routes, gates, w_gate, w_up, w_down, moe_out, norm_gain, out_grad):
    z_count, x_count, t_count = (lax.axis_size(name) for name in AXES)
    plane_size = x_count * t_count
    tok_rows, features = tokens.shape
    capacity = groups * tok_rows // (z_count * plane_size)
    slots = -(-capacity // 16) * 16
    group_rows = 3 * tok_rows // 8
    scratch = fused_scratch(
        tok_rows, features, moe_out.shape[1], w_gate.shape[2], group_rows, z_count, t_count, plane_size, slots
    )
    held = size_of(scratch)
    grads = 3 * 2 * features * w_gate.shape[2]
    if held + grads + 8 * MIB > 64 * MIB:
        return apart(tokens, routes, gates, w_gate, w_up, w_down, moe_out, norm_gain, out_grad)
    token_grad, rows, grad_gate, grad_up, grad_down = fused(
        tokens,
        routes.T,
        gates.T,
        moe_out,
        out_grad,
        norm_gain[None, :],
        w_gate,
        w_up,
        w_down,
        scratch,
        held + 4 * MIB,
        plane_size,
        slots,
        z_count,
        t_count,
    )
    token_grad, gates_grad, grad_gate, grad_up, grad_down = put_out(
        token_grad, rows.astype(jnp.bfloat16), grad_gate, grad_up, grad_down
    )
    return (token_grad, gates_grad.T, grad_gate[None], grad_up[None], grad_down[None])


def solution(mesh):
    ep, tp = mesh.shape["ep"], mesh.shape["tp"]
    cut = Mesh(mesh.devices.reshape(groups, ep // groups, tp), AXES)
    rows, ep_axes = P(AXES, None), ("z", "x")
    cube = P(AXES, None, None)
    return jax.shard_map(
        local,
        mesh=cut,
        in_specs=(rows, rows, rows, cube, cube, cube, P(ep_axes, "tp"), P("tp"), P(ep_axes, "tp")),
        out_specs=(rows, rows, cube, cube, cube),
        check_vma=False,
    )
```

```python
import functools

import jax
import jax.numpy as jnp
from jax import lax
from jax.experimental import pallas as pl
from jax.experimental.pallas import tpu as pltpu
from jax.sharding import Mesh
from jax.sharding import PartitionSpec as P

epsilon = 1e-06
groups = 4
MESH = pl.DeviceIdType.MESH
AXES = ("z", "x", "tp")
META_ROWS = 8
LANES = 128


def contract(left, right, left_dim, right_dim, **kw):
    return lax.dot_general(
        left, right, (((left_dim,), (right_dim,)), ((), ())), preferred_element_type=jnp.float32, **kw
    )


def earlier_equal(ids):
    count = ids.shape[-1]
    place = jnp.arange(count, dtype=jnp.int32)
    same = (ids[..., :, None] == ids[..., None, :]) & (place[:, None] > place[None, :])
    return jnp.sum(same.astype(jnp.int32), axis=-1)


class Place:
    def __init__(self, plane_size):
        self.z, self.x, self.t = (lax.axis_index(name) for name in AXES)
        self.zc, self.tc = lax.axis_size("z"), lax.axis_size("tp")
        self.plane = plane_size
        self.own = self.x * self.tc + self.t

    def at(self, d, k=0):
        return (lax.rem(self.z + d, self.zc), self.x, lax.rem(self.t + k, self.tc))

    def back(self, d):
        return (lax.rem(self.z + self.zc - d, self.zc), self.x, self.t)

    def peer(self, k):
        q = lax.rem(self.own + k, self.plane)
        return q, (self.z, q // self.tc, lax.rem(q, self.tc))


def enter(place, wide):
    wait = greet_all(place, wide)
    wait()


def greet_all(place, wide):
    barrier = pltpu.get_barrier_semaphore()

    def greet(device):
        pl.semaphore_signal(barrier, inc=1, device_id=device, device_id_type=MESH)

    lax.fori_loop(1, place.plane, lambda k, c: (greet(place.peer(k)[1]), c)[1], 0)
    across = place.tc if wide else 1
    for d in range(1, place.zc):
        lax.fori_loop(0, across, lambda k, c: (greet(place.at(d, k)), c)[1], 0)
    return lambda: pl.semaphore_wait(barrier, place.plane - 1 + (place.zc - 1) * across)


def each(first, last, act):
    lax.fori_loop(first, last, lambda k, c: (act(k), c)[1], 0)


def columns(features, act, most=512):
    chunk = min(most, features)
    each(0, features // chunk, lambda c: act(pl.ds(pl.multiple_of(c * chunk, chunk), chunk)))


def iota(shape, dim):
    return lax.broadcasted_iota(jnp.int32, shape, dim)


def chosen(meta, row, slots, width):
    ids = meta[row : row + 1, :width].astype(jnp.int32)
    return iota((slots, width), 0) == ids


def picker(meta, slots, width):
    return (chosen(meta, 0, slots, width) | chosen(meta, 1, slots, width)).astype(
        jnp.float32
    ).astype(jnp.bfloat16)


def dispatch_kernel(
    plane_size, slots, tok_ref, meta_ref, saved_ref, grad_ref, gain_ref,
    tok_out, cot_out, w_out, meta_out,
    mbuf, stat, stbuf, cotz, ztok, zcot, stok, scot, wsend, wrecv,
    ms_sem, mr_sem, ss_sem, sr_sem, zs_sem, zr_sem, ps_sem, pr_sem, loc_sem, ws_sem, wr_sem,
):
    place = Place(plane_size)
    z, x, t, zc, tc = place.z, place.x, place.t, place.zc, place.tc
    own, peer = place.own, place.peer
    features = tok_ref.shape[-1]
    group_rows = tok_ref.shape[1]
    part = saved_ref.shape[-1]
    block = saved_ref.shape[0] // tc
    all_slots = plane_size * slots
    bf16 = jnp.bfloat16
    enter(place, True)

    def rows_of(q):
        return pl.ds(pl.multiple_of(q * slots, slots), slots)

    def remote(src, dst, send, recv, device):
        return pltpu.make_async_remote_copy(
            src_ref=src, dst_ref=dst, send_sem=send, recv_sem=recv, device_id=device, device_id_type=MESH
        )

    def meta_copy(d, k):
        return remote(
            meta_ref.at[lax.rem(z + d, zc)], mbuf.at[d, t], ms_sem.at[d, k], mr_sem.at[d, k], place.at(d, k)
        )

    def stat_copy(k):
        return remote(stat, stbuf.at[k], ss_sem.at[k], sr_sem.at[k], place.at(0, k))

    def z_copy(a, d):
        src, dst = ((tok_ref, ztok), (cotz, zcot))[a]
        return remote(
            src.at[lax.rem(z + d, zc)], dst.at[d], zs_sem.at[a, d], zr_sem.at[a, d], place.at(d)
        )

    def plane_parts(a, d, q):
        if a == 0:
            return stok.at[d, rows_of(q)], tok_out.at[d, rows_of(own)]
        cols = pl.ds(pl.multiple_of(t * part, part), part)
        return scot.at[d, :, rows_of(q)], cot_out.at[d, x, :, :, cols]

    def plane_copy(a, d, k):
        q, device = peer(k)
        src, dst = plane_parts(a, d, q)
        return remote(src, dst, ps_sem.at[a, d, k], pr_sem.at[a, d, k], device)

    def own_copy(a, d):
        src, dst = plane_parts(a, d, own)
        return pltpu.make_async_copy(src, dst, loc_sem.at[a, d])

    def w_copy(k):
        q, device = peer(k)
        return remote(wsend.at[rows_of(q)], wrecv.at[rows_of(own)], ws_sem.at[k], wr_sem.at[k], device)

    def spread_out(a, d):
        each(1, plane_size, lambda k: plane_copy(a, d, k).start())
        own_copy(a, d).start()

    def send_tok(d):
        sel = picker(mbuf[d, t], all_slots, group_rows)

        def one(cols):
            rows = ztok[d, :, cols] if d else tok_ref[z, :, cols]
            stok[d, :, cols] = jnp.dot(sel, rows, preferred_element_type=jnp.float32).astype(bf16)

        columns(features, one)
        spread_out(0, d)

    def send_cot(d):
        for b in range(tc):
            sel = picker(mbuf[d, b], all_slots, group_rows)
            rows = slice(b * group_rows, (b + 1) * group_rows)
            value = zcot[d, rows, :] if d else cotz[z, rows, :]
            scot[d, b] = jnp.dot(sel, value, preferred_element_type=jnp.float32).astype(bf16)
        spread_out(1, d)

    mbuf[0, t] = meta_ref[z]
    for d in range(zc):
        each(0 if d else 1, tc, lambda k: meta_copy(d, k).start())
    for d in range(1, zc):
        z_copy(0, d).start()

    eye = iota((block, block), 0) == iota((block, block), 1)
    gain = gain_ref[...]
    for b in range(tc):
        rows = slice(b * block, (b + 1) * block)
        saved = saved_ref[rows, :].astype(jnp.float32)
        scaled = gain * grad_ref[rows, :].astype(jnp.float32)
        for i, value in enumerate((saved * saved, saved * scaled)):
            total = jnp.sum(value, axis=1, keepdims=True)
            row = i * tc + b
            stat[row : row + 1, :] = jnp.sum(jnp.where(eye, total, 0.0), axis=0, keepdims=True)
    each(1, tc, lambda k: stat_copy(k).start())

    send_tok(0)

    each(1, tc, lambda k: stat_copy(k).wait_recv())
    each(1, tc, lambda k: meta_copy(0, k).wait_recv())
    totals = stat[...]
    for k in range(1, tc):
        totals = totals + stbuf[k]
    inv = lax.rsqrt(totals[:tc] / features + epsilon)
    coef = inv * inv * inv * totals[tc:] / features
    for b in range(tc):
        rows = slice(b * block, (b + 1) * block)
        saved = saved_ref[rows, :].astype(jnp.float32)
        scaled = gain * grad_ref[rows, :].astype(jnp.float32)
        inv_col = jnp.sum(jnp.where(eye, inv[b : b + 1], 0.0), axis=1, keepdims=True)
        coef_col = jnp.sum(jnp.where(eye, coef[b : b + 1], 0.0), axis=1, keepdims=True)
        cot = (inv_col * scaled - saved * coef_col).astype(bf16)
        pack = chosen(mbuf[0, b], 4, zc * group_rows, block).astype(jnp.float32).astype(bf16)
        packed = jnp.dot(pack, cot, preferred_element_type=jnp.float32).astype(bf16)
        for g in range(zc):
            cotz[g, b * group_rows : (b + 1) * group_rows, :] = packed[g * group_rows : (g + 1) * group_rows]
    for d in range(1, zc):
        z_copy(1, d).start()
    send_cot(0)

    for d in range(1, zc):
        each(0, tc, lambda k: meta_copy(d, k).wait_recv())
    weights = jnp.zeros((all_slots, LANES), jnp.float32)
    for d in range(zc):
        meta = mbuf[d, t]
        meta_out[d] = meta
        total = jnp.zeros((all_slots, 1), jnp.float32)
        for i in range(2):
            hit = chosen(meta, i, all_slots, group_rows)
            total = total + jnp.sum(
                jnp.where(hit, meta[2 + i : 3 + i, :group_rows], 0.0), axis=1, keepdims=True
            )
        weights = jnp.where(iota((all_slots, LANES), 1) == d, total, weights)
    wsend[...] = weights.astype(bf16)
    each(1, plane_size, lambda k: w_copy(k).start())
    wrecv[rows_of(own)] = wsend[rows_of(own)]

    for d in range(1, zc):
        z_copy(0, d).wait_recv()
        send_tok(d)
    for d in range(1, zc):
        z_copy(1, d).wait_recv()
        send_cot(d)

    each(1, plane_size, lambda k: w_copy(k).wait_recv())
    w_out[...] = wrecv[...]
    for a in range(2):
        for d in range(zc):
            own_copy(a, d).wait()
            each(1, plane_size, lambda k: plane_copy(a, d, k).wait(), )
            if d:
                z_copy(a, d).wait_send()
    for d in range(zc):
        each(0 if d else 1, tc, lambda k: meta_copy(d, k).wait_send())
    each(1, tc, lambda k: stat_copy(k).wait_send())
    each(1, plane_size, lambda k: w_copy(k).wait_send())


def combine_kernel(
    plane_size, slots, back_ref, gg_ref, meta_ref, out_ref, gout_ref,
    rbuf, cbuf, ggbuf, gbuf, gland, zs_sem, zr_sem, ps_sem, pr_sem, loc_sem, own_sem,
    gs_sem, gr_sem, gzs_sem, gzr_sem,
):
    place = Place(plane_size)
    z, zc, own, peer = place.z, place.zc, place.own, place.peer
    features = back_ref.shape[-1]
    group_rows = out_ref.shape[1]
    all_slots = plane_size * slots
    enter(place, False)

    def rows_of(q):
        return pl.ds(pl.multiple_of(q * slots, slots), slots)

    def remote(src, dst, send, recv, device):
        return pltpu.make_async_remote_copy(
            src_ref=src, dst_ref=dst, send_sem=send, recv_sem=recv, device_id=device, device_id_type=MESH
        )

    def plane_copy(d, k):
        q, device = peer(k)
        return remote(
            back_ref.at[d, rows_of(q)], rbuf.at[d, rows_of(own)], ps_sem.at[d, k], pr_sem.at[d, k], device
        )

    def own_rows(d):
        return pltpu.make_async_copy(back_ref.at[d, rows_of(own)], rbuf.at[d, rows_of(own)], loc_sem.at[d])

    def gg_copy(k):
        q, device = peer(k)
        return remote(gg_ref.at[rows_of(q)], ggbuf.at[rows_of(own)], gs_sem.at[k], gr_sem.at[k], device)

    def z_copy(d):
        return remote(cbuf.at[d], out_ref.at[z], zs_sem.at[d], zr_sem.at[d], place.back(d))

    def gz_copy(d):
        return remote(gbuf.at[d], gland.at[z], gzs_sem.at[d], gzr_sem.at[d], place.back(d))

    keep = pltpu.make_async_copy(cbuf.at[0], out_ref.at[z], own_sem)
    order = list(range(1, zc)) + [0]
    each(1, plane_size, lambda k: gg_copy(k).start())
    ggbuf[rows_of(own)] = gg_ref[rows_of(own)]
    for d in order:
        own_rows(d).start()
        each(1, plane_size, lambda k: plane_copy(d, k).start())
    each(1, plane_size, lambda k: gg_copy(k).wait_recv())
    returned = ggbuf[...].astype(jnp.float32)
    for d in order:
        meta = meta_ref[d]
        column = jnp.sum(
            jnp.where(iota(returned.shape, 1) == d, returned, 0.0), axis=1, keepdims=True
        )
        for i in range(2):
            hit = chosen(meta, i, all_slots, LANES)
            gbuf[d, i : i + 1, :] = jnp.sum(jnp.where(hit, column, 0.0), axis=0, keepdims=True)
        if d:
            gz_copy(d).start()
        else:
            gland[z] = gbuf[0]
    for d in order:
        own_rows(d).wait()
        each(1, plane_size, lambda k: plane_copy(d, k).wait_recv())
        sel = picker(meta_ref[d], all_slots, group_rows)

        def one(cols):
            cbuf[d, :, cols] = contract(sel, rbuf[d, :, cols], 0, 0).astype(cbuf.dtype)

        columns(features, one)
        if d:
            z_copy(d).start()
        else:
            keep.start()
    for d in order:
        each(1, plane_size, lambda k: plane_copy(d, k).wait_send())
        if d:
            gz_copy(d).wait()
            z_copy(d).wait()
    keep.wait()
    gout_ref[...] = gland[...]
    each(1, plane_size, lambda k: gg_copy(k).wait_send())


def vmem():
    return pl.BlockSpec(memory_space=pltpu.VMEM)


def anywhere():
    return pl.BlockSpec(memory_space=pl.ANY)


def dispatch(tok_send, meta, saved, grad, gain, plane_size, slots, tc):
    zc, group_rows, features = tok_send.shape
    part = saved.shape[1]
    rows = plane_size * slots
    bf16 = tok_send.dtype
    dma, struct, space = pltpu.SemaphoreType.DMA, jax.ShapeDtypeStruct, pltpu.VMEM
    f32 = jnp.float32
    return pl.pallas_call(
        functools.partial(dispatch_kernel, plane_size, slots),
        out_shape=(
            struct((zc, rows, features), bf16),
            struct((zc, plane_size // tc, tc, slots, features), bf16),
            struct((rows, LANES), bf16),
            struct(meta.shape, f32),
        ),
        in_specs=[vmem()] * 5,
        out_specs=(anywhere(), anywhere(), vmem(), vmem()),
        scratch_shapes=[
            space((zc, tc, META_ROWS, LANES), f32),
            space((2 * tc, LANES), f32),
            space((tc, 2 * tc, LANES), f32),
            space((zc, tc * group_rows, part), bf16),
            space((zc, group_rows, features), bf16),
            space((zc, tc * group_rows, part), bf16),
            space((zc, rows, features), bf16),
            space((zc, tc, rows, part), bf16),
            space((rows, LANES), bf16),
            space((rows, LANES), bf16),
            dma((zc, tc)),
            dma((zc, tc)),
            dma((tc,)),
            dma((tc,)),
            dma((2, zc)),
            dma((2, zc)),
            dma((2, zc, plane_size)),
            dma((2, zc, plane_size)),
            dma((2, zc)),
            dma((plane_size,)),
            dma((plane_size,)),
        ],
        compiler_params=pltpu.CompilerParams(
            collective_id=0, has_side_effects=True, vmem_limit_bytes=48 * 1024 * 1024
        ),
        name="dispatch",
    )(tok_send, meta, saved, grad, gain)


def combine(back, gg, meta, group_rows, plane_size, slots):
    zc, rows, features = back.shape
    dma, struct, space = pltpu.SemaphoreType.DMA, jax.ShapeDtypeStruct, pltpu.VMEM
    return pl.pallas_call(
        functools.partial(combine_kernel, plane_size, slots),
        out_shape=(struct((zc, group_rows, features), back.dtype), struct(meta.shape, meta.dtype)),
        in_specs=[anywhere(), vmem(), vmem()],
        out_specs=(anywhere(), vmem()),
        scratch_shapes=[
            space(back.shape, back.dtype),
            space((zc, group_rows, features), back.dtype),
            space(gg.shape, gg.dtype),
            space(meta.shape, meta.dtype),
            space(meta.shape, meta.dtype),
            dma((zc,)),
            dma((zc,)),
            dma((zc, plane_size)),
            dma((zc, plane_size)),
            dma((zc,)),
            dma(()),
            dma((plane_size,)),
            dma((plane_size,)),
            dma((zc,)),
            dma((zc,)),
        ],
        compiler_params=pltpu.CompilerParams(
            collective_id=1, has_side_effects=True, vmem_limit_bytes=48 * 1024 * 1024
        ),
        name="combine",
    )(back, gg, meta)


def apart(tokens, routes, gates, w_gate, w_up, w_down, moe_out, norm_gain, out_grad):
    z_count, x_count, t_count = (lax.axis_size(name) for name in AXES)
    plane_size = x_count * t_count
    devices = z_count * plane_size
    tok_rows, features = tokens.shape
    top_count = routes.shape[1]
    capacity = groups * tok_rows // devices
    slots = -(-capacity // 16) * 16
    group_rows = 3 * tok_rows // 8
    rows = plane_size * slots
    bf16, f32 = jnp.bfloat16, jnp.float32

    own_ids = routes.T.reshape(-1)
    own_group = routes[:, 0] // plane_size
    z_slot = own_group * group_rows + earlier_equal(own_group)
    hit = jnp.arange(groups * group_rows, dtype=jnp.int32)[:, None] == z_slot[None, :]
    tok_send = jnp.dot(hit.astype(bf16), tokens, preferred_element_type=f32).astype(bf16)
    slot_of = (own_ids % plane_size) * slots + earlier_equal(own_ids)
    values = jnp.concatenate(
        [
            slot_of.reshape(top_count, tok_rows).astype(f32) + 1.0,
            gates.T.astype(bf16).astype(f32),
        ]
    )
    packed = contract(values, hit.astype(f32), 1, 1, precision=lax.Precision.HIGHEST)
    packed = packed - jnp.array([1.0, 1.0, 0.0, 0.0], f32)[:, None]
    packed = packed.reshape(2 * top_count, groups, group_rows).transpose(1, 0, 2)
    packed = jnp.pad(
        packed,
        ((0, 0), (0, 0), (0, LANES - group_rows)),
        constant_values=-1.0,
    )
    extra = jnp.broadcast_to(z_slot.astype(f32)[None, None, :], (groups, META_ROWS - 4, tok_rows))
    meta = jnp.concatenate([packed, extra], axis=1)

    token_in, cot_in, gate_in, meta_in = dispatch(
        tok_send.reshape(groups, group_rows, features),
        meta,
        moe_out,
        out_grad,
        norm_gain[None, :],
        plane_size,
        slots,
        t_count,
    )
    weight = gate_in[:, :z_count].astype(f32).T.reshape(-1)[:, None]
    row_block = token_in.reshape(devices * slots, features)
    cot_in = cot_in.reshape(devices * slots, features)
    w_gate_one = w_gate[0]
    w_up_one = w_up[0]
    w_down_one = w_down[0]
    pre_gate = jnp.dot(row_block, w_gate_one, preferred_element_type=f32)
    pre_up = jnp.dot(row_block, w_up_one, preferred_element_type=f32)
    sigmoid_gate = jax.nn.sigmoid(pre_gate)
    activated = pre_gate * sigmoid_gate
    hidden = activated * pre_up
    hid_grad = contract(cot_in, w_down_one, 1, 1)
    gate_grad = jnp.sum(hidden * hid_grad, axis=1).astype(bf16)
    d_hidden = weight * hid_grad
    d_gate = (d_hidden * pre_up * sigmoid_gate * (1.0 + pre_gate * (1.0 - sigmoid_gate))).astype(bf16)
    d_up = (d_hidden * activated).astype(bf16)
    token_back = (contract(d_gate, w_gate_one, 1, 1) + contract(d_up, w_up_one, 1, 1)).astype(bf16)
    scaled_cot = (weight * cot_in.astype(f32)).astype(bf16)
    grad_gate = contract(row_block, d_gate, 0, 0).astype(bf16)
    grad_up = contract(row_block, d_up, 0, 0).astype(bf16)
    grad_down = contract(hidden.astype(bf16), scaled_cot, 0, 0).astype(bf16)

    gg = jnp.pad(gate_grad.reshape(z_count, rows).T, ((0, 0), (0, LANES - z_count)))
    back, gback = combine(
        token_back.reshape(z_count, rows, features), gg, meta_in, group_rows, plane_size, slots
    )
    token_grad = contract(hit.astype(bf16), back.reshape(groups * group_rows, features), 0, 0).astype(bf16)
    gvals = gback[:, :top_count, :group_rows].transpose(1, 0, 2).reshape(top_count, groups * group_rows)
    gates_grad = jnp.sum(jnp.where(hit.T[:, None, :], gvals[None], 0.0), axis=2).astype(bf16)
    return (token_grad, gates_grad, grad_gate[None], grad_up[None], grad_down[None])


def fused_kernel(
    plane_size, slots, tok_hbm, route_hbm, gate_hbm, saved_hbm, grad_hbm, gain_hbm, wg_hbm, wu_hbm, wd_hbm,
    tg_ref, gg_out, dwg_ref, dwu_ref, dwd_ref,
    route_ref, gate_ref, gain_ref, tok, saved_ref, grad_ref, wg, wu, wd, meta, mbuf, stat, stbuf, tokz, cotz, ztok, zcot, stok, scot,
    wsend, wrecv, tok_in, cot_in, hid, dg, du, back, rbuf, cbuf, land, ggsend, ggbuf, gbuf, gland,
    in_sem, ms_sem, mr_sem, ss_sem, sr_sem, zs_sem, zr_sem, ps_sem, pr_sem, ws_sem, wr_sem,
    rs_sem, rr_sem, os_sem, or_sem, gs_sem, gr_sem, gzs_sem, gzr_sem,
):
    place = Place(plane_size)
    z, x, t, zc, tc = place.z, place.x, place.t, place.zc, place.tc
    own, peer = place.own, place.peer
    block, features = tok.shape
    part = saved_ref.shape[-1]
    group_rows = tokz.shape[1]
    chunk = plane_size * slots
    width = wg.shape[-1]
    bf16, f32 = jnp.bfloat16, jnp.float32

    loads = [
        pltpu.make_async_copy(src, dst, in_sem.at[i])
        for i, (src, dst) in enumerate(
            (
                (route_hbm, route_ref),
                (gate_hbm, gate_ref),
                (tok_hbm, tok),
                (gain_hbm, gain_ref),
                (saved_hbm, saved_ref),
                (grad_hbm, grad_ref),
                (wg_hbm.at[0], wg),
                (wu_hbm.at[0], wu),
                (wd_hbm.at[0], wd),
            )
        )
    ]
    for load in loads[:6]:
        load.start()
    everyone = greet_all(place, True)

    half, odd = z // (zc // 2), lax.rem(z, 2)

    def apart_from(source):
        return lax.rem(z - source + zc, zc)

    near = apart_from(z + 1 - 2 * odd)
    far = apart_from((zc - 1) * (1 - half))
    late = apart_from(zc // 2 - half)
    sending = [lax.rem(zc - d, zc) for d in (near, far, late)]
    edge = half * odd + (1 - half) * (1 - odd)
    early = edge * far + (1 - edge) * near
    middle = edge * near + (1 - edge) * far

    def rows_of(q):
        return pl.ds(pl.multiple_of(q * slots, slots), slots)

    def whole(d):
        return pl.ds(pl.multiple_of(d * chunk, chunk), chunk)

    def mine(d):
        return isinstance(d, int) and d == 0

    def chunk_rows(d, q):
        return pl.ds(pl.multiple_of(d * chunk + q * slots, slots), slots)

    def remote(src, dst, send, recv, device):
        return pltpu.make_async_remote_copy(
            src_ref=src, dst_ref=dst, send_sem=send, recv_sem=recv, device_id=device, device_id_type=MESH
        )

    def meta_copy(d, k):
        return remote(
            meta.at[lax.rem(z + d, zc)], mbuf.at[d, t], ms_sem.at[d, k], mr_sem.at[d, k], place.at(d, k)
        )

    def stat_copy(k):
        return remote(stat, stbuf.at[k], ss_sem.at[k], sr_sem.at[k], place.at(0, k))

    def z_copy(a, d):
        src, dst = ((tokz, ztok), (cotz, zcot))[a]
        return remote(
            src.at[lax.rem(z + d, zc)], dst.at[d], zs_sem.at[a, d], zr_sem.at[a, d], place.at(d)
        )

    def plane_parts(a, d, q):
        if a == 0:
            return stok.at[d, rows_of(q)], tok_in.at[chunk_rows(d, own)]
        cols = pl.ds(pl.multiple_of(t * part, part), part)
        span = tc * slots
        rows = pl.ds(pl.multiple_of(d * chunk + x * span, span), span)
        return scot.at[d, q], cot_in.at[rows, cols]

    def plane_copy(a, d, k):
        q, device = peer(k)
        src, dst = plane_parts(a, d, q)
        return remote(src, dst, ps_sem.at[a, d, k], pr_sem.at[a, d, k], device)

    def w_copy(k):
        q, device = peer(k)
        return remote(wsend.at[rows_of(q)], wrecv.at[rows_of(own)], ws_sem.at[k], wr_sem.at[k], device)

    def return_copy(d, k):
        q, device = peer(k)
        return remote(
            back.at[d, rows_of(q)], rbuf.at[d, rows_of(own)], rs_sem.at[d, k], rr_sem.at[d, k], device
        )

    def out_copy(d):
        return remote(cbuf.at[d], land.at[own_land], os_sem.at[d], or_sem.at[d], place.back(d))

    own_land = pl.ds(pl.multiple_of(z * group_rows, group_rows), group_rows)

    def gg_copy(k):
        q, device = peer(k)
        return remote(ggsend.at[rows_of(q)], ggbuf.at[rows_of(own)], gs_sem.at[k], gr_sem.at[k], device)

    def gz_copy(d):
        return remote(gbuf.at[d], gland.at[z], gzs_sem.at[d], gzr_sem.at[d], place.back(d))

    def to_peers(copy):
        each(1, plane_size, lambda k: copy(k).start())

    def send_tok(d):
        sel = picker(mbuf[d, t], chunk, group_rows)

        def one(cols):
            rows = tokz[z, :, cols] if mine(d) else ztok[d, :, cols]
            stok[d, :, cols] = jnp.dot(sel, rows, preferred_element_type=f32).astype(bf16)

        columns(features, one, features)
        to_peers(lambda k: plane_copy(0, d, k))
        tok_in[chunk_rows(d, own), :] = stok[d, rows_of(own), :]

    def send_cot(d):
        for b in range(tc):
            sel = picker(mbuf[d, b], chunk, group_rows)
            rows = slice(b * group_rows, (b + 1) * group_rows)
            value = cotz[z, rows, :] if mine(d) else zcot[d, rows, :]
            value = jnp.dot(sel, value, preferred_element_type=f32).astype(bf16)
            for q in range(plane_size):
                scot[d, q, b * slots : (b + 1) * slots, :] = value[q * slots : (q + 1) * slots]
        to_peers(lambda k: plane_copy(1, d, k))
        src, dst = plane_parts(1, d, own)
        dst[...] = src[...]

    eye = iota((block, block), 0) == iota((block, block), 1)
    before = iota((block, block), 0) < iota((block, block), 1)

    def column(row):
        return jnp.sum(jnp.where(eye, row, 0.0), axis=1, keepdims=True)

    def count(mask):
        return jnp.sum(mask.astype(f32), axis=0, keepdims=True)

    loads[0].wait()
    loads[1].wait()
    ids = route_ref[...].astype(f32)
    ids = [ids[i : i + 1] for i in range(2)]
    id_cols = [column(row) for row in ids]
    group = sum((ids[0] >= float(g * plane_size)).astype(f32) for g in range(1, zc))
    z_slot = group * group_rows + count((column(group) == group) & before)
    ranks = [
        count((id_cols[0] == ids[0]) & before),
        count(id_cols[0] == ids[1]) + count((id_cols[1] == ids[1]) & before),
    ]
    values = [(ids[i] - group * plane_size) * slots + ranks[i] + 1.0 for i in range(2)]
    values += [gate_ref[i : i + 1].astype(bf16).astype(f32) for i in range(2)]
    value_cols = [column(row) for row in values]
    slot_col = column(z_slot)
    lane = iota((block, block), 1).astype(f32)
    for g in range(zc):
        hit = (slot_col == lane + float(g * group_rows)) & (lane < float(group_rows))
        for i in range(4):
            row = jnp.sum(jnp.where(hit, value_cols[i], 0.0), axis=0, keepdims=True)
            meta[g, i : i + 1, :] = row - 1.0 if i < 2 else row
        meta[g, 4:8, :] = jnp.broadcast_to(z_slot, (4, block))

    def packer(row):
        slot = iota((zc * group_rows, block), 0).astype(f32)
        return (slot == row).astype(f32).astype(bf16)

    own_pack = packer(z_slot)
    loads[2].wait()

    def pack_tokens(cols):
        value = jnp.dot(own_pack, tok[:, cols], preferred_element_type=f32).astype(bf16)
        for g in range(zc):
            tokz[g, :, cols] = value[g * group_rows : (g + 1) * group_rows]

    columns(features, pack_tokens, features)
    everyone()

    for d in range(zc):
        each(0 if d else 1, tc, lambda k: meta_copy(d, k).start())
    for d in sending:
        z_copy(0, d).start()
    mbuf[0, t] = meta[z]

    for load in loads[6:]:
        load.start()
    for load in loads[3:6]:
        load.wait()
    gain = gain_ref[...]
    for b in range(tc):
        rows = slice(b * block, (b + 1) * block)
        saved = saved_ref[rows, :].astype(f32)
        scaled = gain * grad_ref[rows, :].astype(f32)
        for i, value in enumerate((saved * saved, saved * scaled)):
            total = jnp.sum(value, axis=1, keepdims=True)
            row = i * tc + b
            stat[row : row + 1, :] = jnp.sum(jnp.where(eye, total, 0.0), axis=0, keepdims=True)
    each(1, tc, lambda k: stat_copy(k).start())

    send_tok(0)

    each(1, tc, lambda k: stat_copy(k).wait_recv())
    each(1, tc, lambda k: meta_copy(0, k).wait_recv())
    totals = stat[...]
    for k in range(1, tc):
        totals = totals + stbuf[k]
    inv = lax.rsqrt(totals[:tc] / features + epsilon)
    coef = inv * inv * inv * totals[tc:] / features
    for b in range(tc):
        rows = slice(b * block, (b + 1) * block)
        saved = saved_ref[rows, :].astype(f32)
        scaled = gain * grad_ref[rows, :].astype(f32)
        cot = (column(inv[b : b + 1]) * scaled - saved * column(coef[b : b + 1])).astype(bf16)
        packed = jnp.dot(packer(mbuf[0, b, 4:5, :]), cot, preferred_element_type=f32).astype(bf16)
        for g in range(zc):
            cotz[g, b * group_rows : (b + 1) * group_rows, :] = packed[g * group_rows : (g + 1) * group_rows]
    for d in sending:
        z_copy(1, d).start()
    send_cot(0)

    for d in range(1, zc):
        each(0, tc, lambda k: meta_copy(d, k).wait_recv())
    weights = jnp.zeros((chunk, LANES), f32)
    for d in range(zc):
        tile = mbuf[d, t]
        total = jnp.zeros((chunk, 1), f32)
        for i in range(2):
            hit = chosen(tile, i, chunk, group_rows)
            total = total + jnp.sum(
                jnp.where(hit, tile[2 + i : 3 + i, :group_rows], 0.0), axis=1, keepdims=True
            )
        weights = jnp.where(iota((chunk, LANES), 1) == d, total, weights)
    wsend[...] = weights.astype(bf16)
    to_peers(w_copy)
    wrecv[rows_of(own)] = wsend[rows_of(own)]

    def weight_of(d):
        tile = wrecv[...].astype(f32)
        return jnp.sum(jnp.where(iota(tile.shape, 1) == d, tile, 0.0), axis=1, keepdims=True)

    def compute(d):
        rows = whole(d)
        for a in range(2):
            each(1, plane_size, lambda k: plane_copy(a, d, k).wait_recv())
        weight = weight_of(d)
        step = width

        def forward(c, total):
            cols = pl.ds(pl.multiple_of(c * step, step), step)
            token = tok_in[rows, :]
            pre_gate = jnp.dot(token, wg[:, cols], preferred_element_type=f32)
            pre_up = jnp.dot(token, wu[:, cols], preferred_element_type=f32)
            hid_grad = contract(cot_in[rows, :], wd[cols, :], 1, 1)
            sigmoid = jax.nn.sigmoid(pre_gate)
            activated = pre_gate * sigmoid
            hidden = activated * pre_up
            d_hidden = weight * hid_grad
            hid[rows, cols] = hidden.astype(bf16)
            dg[rows, cols] = (d_hidden * pre_up * sigmoid * (1.0 + pre_gate * (1.0 - sigmoid))).astype(bf16)
            du[rows, cols] = (d_hidden * activated).astype(bf16)
            return total + jnp.sum(hidden * hid_grad, axis=1, keepdims=True)

        total = lax.fori_loop(0, width // step, forward, jnp.zeros((chunk, 1), f32))

        def backward(cols):
            value = contract(dg[rows, :], wg[cols, :], 1, 1) + contract(du[rows, :], wu[cols, :], 1, 1)
            back[d, :, cols] = value.astype(bf16)
            cot_in[rows, cols] = (weight * cot_in[rows, cols].astype(f32)).astype(bf16)

        columns(features, backward, features)
        return total

    def give_back(d):
        to_peers(lambda k: return_copy(d, k))
        rbuf[d, rows_of(own)] = back[d, rows_of(own)]

    def unite(d):
        each(1, plane_size, lambda k: return_copy(d, k).wait_recv())
        sel = picker(mbuf[d, t], chunk, group_rows)

        def one(cols):
            value = contract(sel, rbuf[d, :, cols], 0, 0).astype(bf16)
            if mine(d):
                land[own_land, cols] = value
            else:
                cbuf[d, :, cols] = value

        columns(features, one, features)
        if not mine(d):
            out_copy(d).start()

    def weight_grad(out, left, right):
        step = min(256, out.shape[0])

        def one(c):
            cols = pl.ds(pl.multiple_of(c * step, step), step)
            out[cols, :] = contract(left[:, cols], right[...], 0, 0).astype(bf16)

        each(0, out.shape[0] // step, one)

    def take(a, d):
        z_copy(a, d).wait_recv()
        if a == 0:
            send_tok(d)
        else:
            send_cot(d)

    def note(tile, d):
        return jnp.where(iota((chunk, LANES), 1) == d, compute(d), tile)

    take(0, early)
    take(0, middle)
    for load in loads[6:]:
        load.wait()
    each(1, plane_size, lambda k: w_copy(k).wait_recv())
    tile = note(jnp.zeros((chunk, LANES), f32), 0)
    take(1, early)
    take(1, middle)
    take(0, late)
    tile = note(tile, early)
    take(1, late)
    tile = note(tile, middle)
    give_back(far)
    tile = note(tile, late)
    ggsend[...] = tile.astype(bf16)
    to_peers(gg_copy)
    ggbuf[rows_of(own)] = ggsend[rows_of(own)]
    give_back(late)
    give_back(near)
    give_back(0)
    unite(far)
    weight_grad(dwg_ref, tok_in, dg)
    each(1, plane_size, lambda k: gg_copy(k).wait_recv())
    returned = ggbuf[...].astype(f32)
    for d in range(zc):
        picked = jnp.sum(jnp.where(iota(returned.shape, 1) == d, returned, 0.0), axis=1, keepdims=True)
        for i in range(2):
            hit = chosen(mbuf[d, t], i, chunk, LANES)
            gbuf[d, i : i + 1, :] = jnp.sum(jnp.where(hit, picked, 0.0), axis=0, keepdims=True)
        if d:
            gz_copy(d).start()
    gland[z] = gbuf[0]
    unite(late)
    weight_grad(dwu_ref, tok_in, du)
    unite(near)
    weight_grad(dwd_ref, hid, cot_in)
    for d in range(zc):
        each(0 if d else 1, tc, lambda k: meta_copy(d, k).wait_send())
        for a in range(2):
            each(1, plane_size, lambda k: plane_copy(a, d, k).wait_send())
            if d:
                z_copy(a, d).wait_send()
    each(1, tc, lambda k: stat_copy(k).wait_send())
    each(1, plane_size, lambda k: w_copy(k).wait_send())
    each(1, plane_size, lambda k: gg_copy(k).wait_send())
    for d in range(1, zc):
        gz_copy(d).wait_recv()
    slot_row = mbuf[0, t, 4:5, :]
    for i in range(2):
        row = jnp.zeros((1, block), f32)
        for g in range(zc):
            source = column(gland[g, i : i + 1, :])
            hit = iota((block, block), 0).astype(f32) + float(g * group_rows) == slot_row
            hit = hit & (iota((block, block), 0) < group_rows)
            row = row + jnp.sum(jnp.where(hit, source, 0.0), axis=0, keepdims=True)
        gg_out[i : i + 1, :] = row
    unite(0)
    for d in range(1, zc):
        out_copy(d).wait_recv()

    def unpack(cols):
        tg_ref[:, cols] = contract(own_pack, land[:, cols], 0, 0).astype(bf16)

    columns(features, unpack, features)
    for d in range(zc):
        each(1, plane_size, lambda k: return_copy(d, k).wait_send())
        if d:
            out_copy(d).wait_send()
            gz_copy(d).wait_send()


def fused_scratch(block, features, part, width, group_rows, zc, tc, plane_size, slots):
    bf16, f32, space = jnp.bfloat16, jnp.float32, pltpu.VMEM
    rows = plane_size * slots
    tile = (META_ROWS, LANES)
    return [
        space((2, block), jnp.int32),
        space((2, block), f32),
        space((1, part), f32),
        space((block, features), bf16),
        space((tc * block, part), bf16),
        space((tc * block, part), bf16),
        space((features, width), bf16),
        space((features, width), bf16),
        space((width, features), bf16),
        space((zc,) + tile, f32),
        space((zc, tc) + tile, f32),
        space((2 * tc, LANES), f32),
        space((tc, 2 * tc, LANES), f32),
        space((zc, group_rows, features), bf16),
        space((zc, tc * group_rows, part), bf16),
        space((zc, group_rows, features), bf16),
        space((zc, tc * group_rows, part), bf16),
        space((zc, rows, features), bf16),
        space((zc, plane_size, tc * slots, part), bf16),
        space((rows, LANES), bf16),
        space((rows, LANES), bf16),
        space((zc * rows, features), bf16),
        space((zc * rows, features), bf16),
        space((zc * rows, width), bf16),
        space((zc * rows, width), bf16),
        space((zc * rows, width), bf16),
        space((zc, rows, features), bf16),
        space((zc, rows, features), bf16),
        space((zc, group_rows, features), bf16),
        space((zc * group_rows, features), bf16),
        space((rows, LANES), bf16),
        space((rows, LANES), bf16),
        space((zc,) + tile, f32),
        space((zc,) + tile, f32),
    ]


def fused(tokens, routes, gates, saved, grad, gain, w_gate, w_up, w_down, scratch, limit, plane_size, slots, zc, tc):
    dma, struct = pltpu.SemaphoreType.DMA, jax.ShapeDtypeStruct
    bf16, f32 = jnp.bfloat16, jnp.float32
    semaphores = [
        dma((9,)),
        dma((zc, tc)),
        dma((zc, tc)),
        dma((tc,)),
        dma((tc,)),
        dma((2, zc)),
        dma((2, zc)),
        dma((2, zc, plane_size)),
        dma((2, zc, plane_size)),
        dma((plane_size,)),
        dma((plane_size,)),
        dma((zc, plane_size)),
        dma((zc, plane_size)),
        dma((zc,)),
        dma((zc,)),
        dma((plane_size,)),
        dma((plane_size,)),
        dma((zc,)),
        dma((zc,)),
    ]
    operands = (tokens, routes, gates, saved, grad, gain, w_gate, w_up, w_down)
    space = pltpu.MemorySpace.HBM
    hbm = pl.BlockSpec(memory_space=space)
    return pl.pallas_call(
        functools.partial(fused_kernel, plane_size, slots),
        out_shape=(
            struct(tokens.shape, bf16),
            struct(routes.shape, f32),
            struct(w_gate.shape[1:], bf16),
            struct(w_up.shape[1:], bf16),
            struct(w_down.shape[1:], bf16),
        ),
        in_specs=[hbm] * 9,
        out_specs=(vmem(),) * 5,
        scratch_shapes=scratch + semaphores,
        compiler_params=pltpu.CompilerParams(
            collective_id=2, has_side_effects=True, vmem_limit_bytes=limit
        ),
        name="layer",
    )(*(pltpu.with_memory_space_constraint(value, space) for value in operands))


def size_of(refs):
    total = 0
    for ref in refs:
        count = ref.dtype.itemsize if hasattr(ref.dtype, "itemsize") else jnp.dtype(ref.dtype).itemsize
        for extent in ref.shape:
            count *= extent
        total += count
    return total


MIB = 1024 * 1024


def put_kernel(*refs):
    count = len(refs) // 2
    copies = [pltpu.make_async_copy(refs[i], refs[count + i], refs[-1].at[i]) for i in range(count)]
    for copy in copies:
        copy.start()
    for copy in copies:
        copy.wait()


def put_out(*values):
    return pl.pallas_call(
        put_kernel,
        out_shape=tuple(jax.ShapeDtypeStruct(value.shape, value.dtype) for value in values),
        in_specs=[vmem()] * len(values),
        out_specs=(anywhere(),) * len(values),
        scratch_shapes=[pltpu.SemaphoreType.DMA((len(values),))],
        compiler_params=pltpu.CompilerParams(vmem_limit_bytes=MIB),
        name="put",
    )(*values)


def local(tokens, routes, gates, w_gate, w_up, w_down, moe_out, norm_gain, out_grad):
    z_count, x_count, t_count = (lax.axis_size(name) for name in AXES)
    plane_size = x_count * t_count
    tok_rows, features = tokens.shape
    capacity = groups * tok_rows // (z_count * plane_size)
    slots = -(-capacity // 16) * 16
    group_rows = 3 * tok_rows // 8
    scratch = fused_scratch(
        tok_rows, features, moe_out.shape[1], w_gate.shape[2], group_rows, z_count, t_count, plane_size, slots
    )
    held = size_of(scratch)
    grads = 3 * 2 * features * w_gate.shape[2]
    if held + grads + 8 * MIB > 64 * MIB:
        return apart(tokens, routes, gates, w_gate, w_up, w_down, moe_out, norm_gain, out_grad)
    token_grad, rows, grad_gate, grad_up, grad_down = fused(
        tokens,
        routes.T,
        gates.T,
        moe_out,
        out_grad,
        norm_gain[None, :],
        w_gate,
        w_up,
        w_down,
        scratch,
        held + 4 * MIB,
        plane_size,
        slots,
        z_count,
        t_count,
    )
    token_grad, gates_grad, grad_gate, grad_up, grad_down = put_out(
        token_grad, rows.astype(jnp.bfloat16), grad_gate, grad_up, grad_down
    )
    return (token_grad, gates_grad.T, grad_gate[None], grad_up[None], grad_down[None])


def solution(mesh):
    ep, tp = mesh.shape["ep"], mesh.shape["tp"]
    cut = Mesh(mesh.devices.reshape(groups, ep // groups, tp), AXES)
    rows, ep_axes = P(AXES, None), ("z", "x")
    cube = P(AXES, None, None)
    return jax.shard_map(
        local,
        mesh=cut,
        in_specs=(rows, rows, rows, cube, cube, cube, P(ep_axes, "tp"), P("tp"), P(ep_axes, "tp")),
        out_specs=(rows, rows, cube, cube, cube),
        check_vma=False,
    )
```

```python
import functools

import jax
import jax.numpy as jnp
from jax import lax
from jax.experimental import pallas as pl
from jax.experimental.pallas import tpu as pltpu
from jax.sharding import Mesh
from jax.sharding import PartitionSpec as P

epsilon = 1e-06
groups = 4
MESH = pl.DeviceIdType.MESH
AXES = ("z", "x", "tp")
META_ROWS = 8
LANES = 128


def contract(left, right, left_dim, right_dim, **kw):
    return lax.dot_general(
        left, right, (((left_dim,), (right_dim,)), ((), ())), preferred_element_type=jnp.float32, **kw
    )


def earlier_equal(ids):
    count = ids.shape[-1]
    place = jnp.arange(count, dtype=jnp.int32)
    same = (ids[..., :, None] == ids[..., None, :]) & (place[:, None] > place[None, :])
    return jnp.sum(same.astype(jnp.int32), axis=-1)


class Place:
    def __init__(self, plane_size):
        self.z, self.x, self.t = (lax.axis_index(name) for name in AXES)
        self.zc, self.tc = lax.axis_size("z"), lax.axis_size("tp")
        self.plane = plane_size
        self.own = self.x * self.tc + self.t

    def at(self, d, k=0):
        return (lax.rem(self.z + d, self.zc), self.x, lax.rem(self.t + k, self.tc))

    def back(self, d):
        return (lax.rem(self.z + self.zc - d, self.zc), self.x, self.t)

    def peer(self, k):
        q = lax.rem(self.own + k, self.plane)
        return q, (self.z, q // self.tc, lax.rem(q, self.tc))


def enter(place, wide):
    wait = greet_all(place, wide)
    wait()


def greet_all(place, wide):
    barrier = pltpu.get_barrier_semaphore()

    def greet(device):
        pl.semaphore_signal(barrier, inc=1, device_id=device, device_id_type=MESH)

    lax.fori_loop(1, place.plane, lambda k, c: (greet(place.peer(k)[1]), c)[1], 0)
    across = place.tc if wide else 1
    for d in range(1, place.zc):
        lax.fori_loop(0, across, lambda k, c: (greet(place.at(d, k)), c)[1], 0)
    return lambda: pl.semaphore_wait(barrier, place.plane - 1 + (place.zc - 1) * across)


def each(first, last, act):
    lax.fori_loop(first, last, lambda k, c: (act(k), c)[1], 0)


def columns(features, act, most=512):
    chunk = min(most, features)
    each(0, features // chunk, lambda c: act(pl.ds(pl.multiple_of(c * chunk, chunk), chunk)))


def iota(shape, dim):
    return lax.broadcasted_iota(jnp.int32, shape, dim)


def chosen(meta, row, slots, width):
    ids = meta[row : row + 1, :width].astype(jnp.int32)
    return iota((slots, width), 0) == ids


def picker(meta, slots, width):
    return (chosen(meta, 0, slots, width) | chosen(meta, 1, slots, width)).astype(
        jnp.float32
    ).astype(jnp.bfloat16)


def dispatch_kernel(
    plane_size, slots, tok_ref, meta_ref, saved_ref, grad_ref, gain_ref,
    tok_out, cot_out, w_out, meta_out,
    mbuf, stat, stbuf, cotz, ztok, zcot, stok, scot, wsend, wrecv,
    ms_sem, mr_sem, ss_sem, sr_sem, zs_sem, zr_sem, ps_sem, pr_sem, loc_sem, ws_sem, wr_sem,
):
    place = Place(plane_size)
    z, x, t, zc, tc = place.z, place.x, place.t, place.zc, place.tc
    own, peer = place.own, place.peer
    features = tok_ref.shape[-1]
    group_rows = tok_ref.shape[1]
    part = saved_ref.shape[-1]
    block = saved_ref.shape[0] // tc
    all_slots = plane_size * slots
    bf16 = jnp.bfloat16
    enter(place, True)

    def rows_of(q):
        return pl.ds(pl.multiple_of(q * slots, slots), slots)

    def remote(src, dst, send, recv, device):
        return pltpu.make_async_remote_copy(
            src_ref=src, dst_ref=dst, send_sem=send, recv_sem=recv, device_id=device, device_id_type=MESH
        )

    def meta_copy(d, k):
        return remote(
            meta_ref.at[lax.rem(z + d, zc)], mbuf.at[d, t], ms_sem.at[d, k], mr_sem.at[d, k], place.at(d, k)
        )

    def stat_copy(k):
        return remote(stat, stbuf.at[k], ss_sem.at[k], sr_sem.at[k], place.at(0, k))

    def z_copy(a, d):
        src, dst = ((tok_ref, ztok), (cotz, zcot))[a]
        return remote(
            src.at[lax.rem(z + d, zc)], dst.at[d], zs_sem.at[a, d], zr_sem.at[a, d], place.at(d)
        )

    def plane_parts(a, d, q):
        if a == 0:
            return stok.at[d, rows_of(q)], tok_out.at[d, rows_of(own)]
        cols = pl.ds(pl.multiple_of(t * part, part), part)
        return scot.at[d, :, rows_of(q)], cot_out.at[d, x, :, :, cols]

    def plane_copy(a, d, k):
        q, device = peer(k)
        src, dst = plane_parts(a, d, q)
        return remote(src, dst, ps_sem.at[a, d, k], pr_sem.at[a, d, k], device)

    def own_copy(a, d):
        src, dst = plane_parts(a, d, own)
        return pltpu.make_async_copy(src, dst, loc_sem.at[a, d])

    def w_copy(k):
        q, device = peer(k)
        return remote(wsend.at[rows_of(q)], wrecv.at[rows_of(own)], ws_sem.at[k], wr_sem.at[k], device)

    def spread_out(a, d):
        each(1, plane_size, lambda k: plane_copy(a, d, k).start())
        own_copy(a, d).start()

    def send_tok(d):
        sel = picker(mbuf[d, t], all_slots, group_rows)

        def one(cols):
            rows = ztok[d, :, cols] if d else tok_ref[z, :, cols]
            stok[d, :, cols] = jnp.dot(sel, rows, preferred_element_type=jnp.float32).astype(bf16)

        columns(features, one)
        spread_out(0, d)

    def send_cot(d):
        for b in range(tc):
            sel = picker(mbuf[d, b], all_slots, group_rows)
            rows = slice(b * group_rows, (b + 1) * group_rows)
            value = zcot[d, rows, :] if d else cotz[z, rows, :]
            scot[d, b] = jnp.dot(sel, value, preferred_element_type=jnp.float32).astype(bf16)
        spread_out(1, d)

    mbuf[0, t] = meta_ref[z]
    for d in range(zc):
        each(0 if d else 1, tc, lambda k: meta_copy(d, k).start())
    for d in range(1, zc):
        z_copy(0, d).start()

    eye = iota((block, block), 0) == iota((block, block), 1)
    gain = gain_ref[...]
    for b in range(tc):
        rows = slice(b * block, (b + 1) * block)
        saved = saved_ref[rows, :].astype(jnp.float32)
        scaled = gain * grad_ref[rows, :].astype(jnp.float32)
        for i, value in enumerate((saved * saved, saved * scaled)):
            total = jnp.sum(value, axis=1, keepdims=True)
            row = i * tc + b
            stat[row : row + 1, :] = jnp.sum(jnp.where(eye, total, 0.0), axis=0, keepdims=True)
    each(1, tc, lambda k: stat_copy(k).start())

    send_tok(0)

    each(1, tc, lambda k: stat_copy(k).wait_recv())
    each(1, tc, lambda k: meta_copy(0, k).wait_recv())
    totals = stat[...]
    for k in range(1, tc):
        totals = totals + stbuf[k]
    inv = lax.rsqrt(totals[:tc] / features + epsilon)
    coef = inv * inv * inv * totals[tc:] / features
    for b in range(tc):
        rows = slice(b * block, (b + 1) * block)
        saved = saved_ref[rows, :].astype(jnp.float32)
        scaled = gain * grad_ref[rows, :].astype(jnp.float32)
        inv_col = jnp.sum(jnp.where(eye, inv[b : b + 1], 0.0), axis=1, keepdims=True)
        coef_col = jnp.sum(jnp.where(eye, coef[b : b + 1], 0.0), axis=1, keepdims=True)
        cot = (inv_col * scaled - saved * coef_col).astype(bf16)
        pack = chosen(mbuf[0, b], 4, zc * group_rows, block).astype(jnp.float32).astype(bf16)
        packed = jnp.dot(pack, cot, preferred_element_type=jnp.float32).astype(bf16)
        for g in range(zc):
            cotz[g, b * group_rows : (b + 1) * group_rows, :] = packed[g * group_rows : (g + 1) * group_rows]
    for d in range(1, zc):
        z_copy(1, d).start()
    send_cot(0)

    for d in range(1, zc):
        each(0, tc, lambda k: meta_copy(d, k).wait_recv())
    weights = jnp.zeros((all_slots, LANES), jnp.float32)
    for d in range(zc):
        meta = mbuf[d, t]
        meta_out[d] = meta
        total = jnp.zeros((all_slots, 1), jnp.float32)
        for i in range(2):
            hit = chosen(meta, i, all_slots, group_rows)
            total = total + jnp.sum(
                jnp.where(hit, meta[2 + i : 3 + i, :group_rows], 0.0), axis=1, keepdims=True
            )
        weights = jnp.where(iota((all_slots, LANES), 1) == d, total, weights)
    wsend[...] = weights.astype(bf16)
    each(1, plane_size, lambda k: w_copy(k).start())
    wrecv[rows_of(own)] = wsend[rows_of(own)]

    for d in range(1, zc):
        z_copy(0, d).wait_recv()
        send_tok(d)
    for d in range(1, zc):
        z_copy(1, d).wait_recv()
        send_cot(d)

    each(1, plane_size, lambda k: w_copy(k).wait_recv())
    w_out[...] = wrecv[...]
    for a in range(2):
        for d in range(zc):
            own_copy(a, d).wait()
            each(1, plane_size, lambda k: plane_copy(a, d, k).wait(), )
            if d:
                z_copy(a, d).wait_send()
    for d in range(zc):
        each(0 if d else 1, tc, lambda k: meta_copy(d, k).wait_send())
    each(1, tc, lambda k: stat_copy(k).wait_send())
    each(1, plane_size, lambda k: w_copy(k).wait_send())


def combine_kernel(
    plane_size, slots, back_ref, gg_ref, meta_ref, out_ref, gout_ref,
    rbuf, cbuf, ggbuf, gbuf, gland, zs_sem, zr_sem, ps_sem, pr_sem, loc_sem, own_sem,
    gs_sem, gr_sem, gzs_sem, gzr_sem,
):
    place = Place(plane_size)
    z, zc, own, peer = place.z, place.zc, place.own, place.peer
    features = back_ref.shape[-1]
    group_rows = out_ref.shape[1]
    all_slots = plane_size * slots
    enter(place, False)

    def rows_of(q):
        return pl.ds(pl.multiple_of(q * slots, slots), slots)

    def remote(src, dst, send, recv, device):
        return pltpu.make_async_remote_copy(
            src_ref=src, dst_ref=dst, send_sem=send, recv_sem=recv, device_id=device, device_id_type=MESH
        )

    def plane_copy(d, k):
        q, device = peer(k)
        return remote(
            back_ref.at[d, rows_of(q)], rbuf.at[d, rows_of(own)], ps_sem.at[d, k], pr_sem.at[d, k], device
        )

    def own_rows(d):
        return pltpu.make_async_copy(back_ref.at[d, rows_of(own)], rbuf.at[d, rows_of(own)], loc_sem.at[d])

    def gg_copy(k):
        q, device = peer(k)
        return remote(gg_ref.at[rows_of(q)], ggbuf.at[rows_of(own)], gs_sem.at[k], gr_sem.at[k], device)

    def z_copy(d):
        return remote(cbuf.at[d], out_ref.at[z], zs_sem.at[d], zr_sem.at[d], place.back(d))

    def gz_copy(d):
        return remote(gbuf.at[d], gland.at[z], gzs_sem.at[d], gzr_sem.at[d], place.back(d))

    keep = pltpu.make_async_copy(cbuf.at[0], out_ref.at[z], own_sem)
    order = list(range(1, zc)) + [0]
    each(1, plane_size, lambda k: gg_copy(k).start())
    ggbuf[rows_of(own)] = gg_ref[rows_of(own)]
    for d in order:
        own_rows(d).start()
        each(1, plane_size, lambda k: plane_copy(d, k).start())
    each(1, plane_size, lambda k: gg_copy(k).wait_recv())
    returned = ggbuf[...].astype(jnp.float32)
    for d in order:
        meta = meta_ref[d]
        column = jnp.sum(
            jnp.where(iota(returned.shape, 1) == d, returned, 0.0), axis=1, keepdims=True
        )
        for i in range(2):
            hit = chosen(meta, i, all_slots, LANES)
            gbuf[d, i : i + 1, :] = jnp.sum(jnp.where(hit, column, 0.0), axis=0, keepdims=True)
        if d:
            gz_copy(d).start()
        else:
            gland[z] = gbuf[0]
    for d in order:
        own_rows(d).wait()
        each(1, plane_size, lambda k: plane_copy(d, k).wait_recv())
        sel = picker(meta_ref[d], all_slots, group_rows)

        def one(cols):
            cbuf[d, :, cols] = contract(sel, rbuf[d, :, cols], 0, 0).astype(cbuf.dtype)

        columns(features, one)
        if d:
            z_copy(d).start()
        else:
            keep.start()
    for d in order:
        each(1, plane_size, lambda k: plane_copy(d, k).wait_send())
        if d:
            gz_copy(d).wait()
            z_copy(d).wait()
    keep.wait()
    gout_ref[...] = gland[...]
    each(1, plane_size, lambda k: gg_copy(k).wait_send())


def vmem():
    return pl.BlockSpec(memory_space=pltpu.VMEM)


def anywhere():
    return pl.BlockSpec(memory_space=pl.ANY)


def dispatch(tok_send, meta, saved, grad, gain, plane_size, slots, tc):
    zc, group_rows, features = tok_send.shape
    part = saved.shape[1]
    rows = plane_size * slots
    bf16 = tok_send.dtype
    dma, struct, space = pltpu.SemaphoreType.DMA, jax.ShapeDtypeStruct, pltpu.VMEM
    f32 = jnp.float32
    return pl.pallas_call(
        functools.partial(dispatch_kernel, plane_size, slots),
        out_shape=(
            struct((zc, rows, features), bf16),
            struct((zc, plane_size // tc, tc, slots, features), bf16),
            struct((rows, LANES), bf16),
            struct(meta.shape, f32),
        ),
        in_specs=[vmem()] * 5,
        out_specs=(anywhere(), anywhere(), vmem(), vmem()),
        scratch_shapes=[
            space((zc, tc, META_ROWS, LANES), f32),
            space((2 * tc, LANES), f32),
            space((tc, 2 * tc, LANES), f32),
            space((zc, tc * group_rows, part), bf16),
            space((zc, group_rows, features), bf16),
            space((zc, tc * group_rows, part), bf16),
            space((zc, rows, features), bf16),
            space((zc, tc, rows, part), bf16),
            space((rows, LANES), bf16),
            space((rows, LANES), bf16),
            dma((zc, tc)),
            dma((zc, tc)),
            dma((tc,)),
            dma((tc,)),
            dma((2, zc)),
            dma((2, zc)),
            dma((2, zc, plane_size)),
            dma((2, zc, plane_size)),
            dma((2, zc)),
            dma((plane_size,)),
            dma((plane_size,)),
        ],
        compiler_params=pltpu.CompilerParams(
            collective_id=0, has_side_effects=True, vmem_limit_bytes=48 * 1024 * 1024
        ),
        name="dispatch",
    )(tok_send, meta, saved, grad, gain)


def combine(back, gg, meta, group_rows, plane_size, slots):
    zc, rows, features = back.shape
    dma, struct, space = pltpu.SemaphoreType.DMA, jax.ShapeDtypeStruct, pltpu.VMEM
    return pl.pallas_call(
        functools.partial(combine_kernel, plane_size, slots),
        out_shape=(struct((zc, group_rows, features), back.dtype), struct(meta.shape, meta.dtype)),
        in_specs=[anywhere(), vmem(), vmem()],
        out_specs=(anywhere(), vmem()),
        scratch_shapes=[
            space(back.shape, back.dtype),
            space((zc, group_rows, features), back.dtype),
            space(gg.shape, gg.dtype),
            space(meta.shape, meta.dtype),
            space(meta.shape, meta.dtype),
            dma((zc,)),
            dma((zc,)),
            dma((zc, plane_size)),
            dma((zc, plane_size)),
            dma((zc,)),
            dma(()),
            dma((plane_size,)),
            dma((plane_size,)),
            dma((zc,)),
            dma((zc,)),
        ],
        compiler_params=pltpu.CompilerParams(
            collective_id=1, has_side_effects=True, vmem_limit_bytes=48 * 1024 * 1024
        ),
        name="combine",
    )(back, gg, meta)


def apart(tokens, routes, gates, w_gate, w_up, w_down, moe_out, norm_gain, out_grad):
    z_count, x_count, t_count = (lax.axis_size(name) for name in AXES)
    plane_size = x_count * t_count
    devices = z_count * plane_size
    tok_rows, features = tokens.shape
    top_count = routes.shape[1]
    capacity = groups * tok_rows // devices
    slots = -(-capacity // 16) * 16
    group_rows = 3 * tok_rows // 8
    rows = plane_size * slots
    bf16, f32 = jnp.bfloat16, jnp.float32

    own_ids = routes.T.reshape(-1)
    own_group = routes[:, 0] // plane_size
    z_slot = own_group * group_rows + earlier_equal(own_group)
    hit = jnp.arange(groups * group_rows, dtype=jnp.int32)[:, None] == z_slot[None, :]
    tok_send = jnp.dot(hit.astype(bf16), tokens, preferred_element_type=f32).astype(bf16)
    slot_of = (own_ids % plane_size) * slots + earlier_equal(own_ids)
    values = jnp.concatenate(
        [
            slot_of.reshape(top_count, tok_rows).astype(f32) + 1.0,
            gates.T.astype(bf16).astype(f32),
        ]
    )
    packed = contract(values, hit.astype(f32), 1, 1, precision=lax.Precision.HIGHEST)
    packed = packed - jnp.array([1.0, 1.0, 0.0, 0.0], f32)[:, None]
    packed = packed.reshape(2 * top_count, groups, group_rows).transpose(1, 0, 2)
    packed = jnp.pad(
        packed,
        ((0, 0), (0, 0), (0, LANES - group_rows)),
        constant_values=-1.0,
    )
    extra = jnp.broadcast_to(z_slot.astype(f32)[None, None, :], (groups, META_ROWS - 4, tok_rows))
    meta = jnp.concatenate([packed, extra], axis=1)

    token_in, cot_in, gate_in, meta_in = dispatch(
        tok_send.reshape(groups, group_rows, features),
        meta,
        moe_out,
        out_grad,
        norm_gain[None, :],
        plane_size,
        slots,
        t_count,
    )
    weight = gate_in[:, :z_count].astype(f32).T.reshape(-1)[:, None]
    row_block = token_in.reshape(devices * slots, features)
    cot_in = cot_in.reshape(devices * slots, features)
    w_gate_one = w_gate[0]
    w_up_one = w_up[0]
    w_down_one = w_down[0]
    pre_gate = jnp.dot(row_block, w_gate_one, preferred_element_type=f32)
    pre_up = jnp.dot(row_block, w_up_one, preferred_element_type=f32)
    sigmoid_gate = jax.nn.sigmoid(pre_gate)
    activated = pre_gate * sigmoid_gate
    hidden = activated * pre_up
    hid_grad = contract(cot_in, w_down_one, 1, 1)
    gate_grad = jnp.sum(hidden * hid_grad, axis=1).astype(bf16)
    d_hidden = weight * hid_grad
    d_gate = (d_hidden * pre_up * sigmoid_gate * (1.0 + pre_gate * (1.0 - sigmoid_gate))).astype(bf16)
    d_up = (d_hidden * activated).astype(bf16)
    token_back = (contract(d_gate, w_gate_one, 1, 1) + contract(d_up, w_up_one, 1, 1)).astype(bf16)
    scaled_cot = (weight * cot_in.astype(f32)).astype(bf16)
    grad_gate = contract(row_block, d_gate, 0, 0).astype(bf16)
    grad_up = contract(row_block, d_up, 0, 0).astype(bf16)
    grad_down = contract(hidden.astype(bf16), scaled_cot, 0, 0).astype(bf16)

    gg = jnp.pad(gate_grad.reshape(z_count, rows).T, ((0, 0), (0, LANES - z_count)))
    back, gback = combine(
        token_back.reshape(z_count, rows, features), gg, meta_in, group_rows, plane_size, slots
    )
    token_grad = contract(hit.astype(bf16), back.reshape(groups * group_rows, features), 0, 0).astype(bf16)
    gvals = gback[:, :top_count, :group_rows].transpose(1, 0, 2).reshape(top_count, groups * group_rows)
    gates_grad = jnp.sum(jnp.where(hit.T[:, None, :], gvals[None], 0.0), axis=2).astype(bf16)
    return (token_grad, gates_grad, grad_gate[None], grad_up[None], grad_down[None])


def fused_kernel(
    plane_size, slots, tok_hbm, route_hbm, gate_hbm, saved_hbm, grad_hbm, gain_hbm, wg_hbm, wu_hbm, wd_hbm,
    tg_ref, gg_out, dwg_ref, dwu_ref, dwd_ref,
    route_ref, gate_ref, gain_ref, tok, saved_ref, grad_ref, wg, wu, wd, meta, mbuf, stat, stbuf, tokz, cotz, ztok, zcot, stok, scot,
    wsend, wrecv, tok_in, cot_in, hid, dg, du, back, rbuf, cbuf, land, ggsend, ggbuf, gbuf, gland,
    in_sem, ms_sem, mr_sem, ss_sem, sr_sem, zs_sem, zr_sem, ps_sem, pr_sem, ws_sem, wr_sem,
    rs_sem, rr_sem, os_sem, or_sem, gs_sem, gr_sem, gzs_sem, gzr_sem,
):
    place = Place(plane_size)
    z, x, t, zc, tc = place.z, place.x, place.t, place.zc, place.tc
    own = place.own

    def peer(k):
        q, bit, rest = 0, 1, plane_size - k
        while bit < plane_size:
            flip = lax.rem(own // bit + rest // bit, 2)
            q, bit = q + flip * bit, bit * 2
        return q, (z, q // tc, lax.rem(q, tc))

    block, features = tok.shape
    part = saved_ref.shape[-1]
    group_rows = tokz.shape[1]
    chunk = plane_size * slots
    width = wg.shape[-1]
    bf16, f32 = jnp.bfloat16, jnp.float32

    loads = [
        pltpu.make_async_copy(src, dst, in_sem.at[i])
        for i, (src, dst) in enumerate(
            (
                (route_hbm, route_ref),
                (gate_hbm, gate_ref),
                (tok_hbm, tok),
                (gain_hbm, gain_ref),
                (saved_hbm, saved_ref),
                (grad_hbm, grad_ref),
                (wg_hbm.at[0], wg),
                (wu_hbm.at[0], wu),
                (wd_hbm.at[0], wd),
            )
        )
    ]
    for load in loads[:6]:
        load.start()
    everyone = greet_all(place, True)

    half, odd = z // (zc // 2), lax.rem(z, 2)

    def apart_from(source):
        return lax.rem(z - source + zc, zc)

    near = apart_from(z + 1 - 2 * odd)
    far = apart_from((zc - 1) * (1 - half))
    late = apart_from(zc // 2 - half)
    sending = [lax.rem(zc - d, zc) for d in (near, far, late)]
    edge = half * odd + (1 - half) * (1 - odd)
    early = edge * far + (1 - edge) * near
    middle = edge * near + (1 - edge) * far

    def rows_of(q):
        return pl.ds(pl.multiple_of(q * slots, slots), slots)

    def whole(d):
        return pl.ds(pl.multiple_of(d * chunk, chunk), chunk)

    def mine(d):
        return isinstance(d, int) and d == 0

    def chunk_rows(d, q):
        return pl.ds(pl.multiple_of(d * chunk + q * slots, slots), slots)

    def remote(src, dst, send, recv, device):
        return pltpu.make_async_remote_copy(
            src_ref=src, dst_ref=dst, send_sem=send, recv_sem=recv, device_id=device, device_id_type=MESH
        )

    def meta_copy(d, k):
        return remote(
            meta.at[lax.rem(z + d, zc)], mbuf.at[d, t], ms_sem.at[d, k], mr_sem.at[d, k], place.at(d, k)
        )

    def stat_copy(k):
        return remote(stat, stbuf.at[k], ss_sem.at[k], sr_sem.at[k], place.at(0, k))

    def z_copy(a, d):
        src, dst = ((tokz, ztok), (cotz, zcot))[a]
        return remote(
            src.at[lax.rem(z + d, zc)], dst.at[d], zs_sem.at[a, d], zr_sem.at[a, d], place.at(d)
        )

    def plane_parts(a, d, q):
        if a == 0:
            return stok.at[d, rows_of(q)], tok_in.at[chunk_rows(d, own)]
        cols = pl.ds(pl.multiple_of(t * part, part), part)
        span = tc * slots
        rows = pl.ds(pl.multiple_of(d * chunk + x * span, span), span)
        return scot.at[d, q], cot_in.at[rows, cols]

    def plane_copy(a, d, k):
        q, device = peer(k)
        src, dst = plane_parts(a, d, q)
        return remote(src, dst, ps_sem.at[a, d, k], pr_sem.at[a, d, k], device)

    def w_copy(k):
        q, device = peer(k)
        return remote(wsend.at[rows_of(q)], wrecv.at[rows_of(own)], ws_sem.at[k], wr_sem.at[k], device)

    def return_copy(d, k, piece=0):
        q, device = peer(k)
        if mine(d):
            cols = pl.ds(piece * (features // 2), features // 2)
            src, dst = back.at[d, rows_of(q), cols], rbuf.at[d, rows_of(own), cols]
        else:
            src, dst = back.at[d, rows_of(q)], rbuf.at[d, rows_of(own)]
        sem = zc if piece else d
        return remote(src, dst, rs_sem.at[sem, k], rr_sem.at[sem, k], device)

    def out_copy(d):
        return remote(cbuf.at[d], land.at[own_land], os_sem.at[d], or_sem.at[d], place.back(d))

    own_land = pl.ds(pl.multiple_of(z * group_rows, group_rows), group_rows)

    def gg_copy(k):
        q, device = peer(k)
        return remote(ggsend.at[rows_of(q)], ggbuf.at[rows_of(own)], gs_sem.at[k], gr_sem.at[k], device)

    def gz_copy(d):
        return remote(gbuf.at[d], gland.at[z], gzs_sem.at[d], gzr_sem.at[d], place.back(d))

    def to_peers(copy):
        each(1, plane_size, lambda k: copy(k).start())

    def send_tok(d):
        sel = picker(mbuf[d, t], chunk, group_rows)

        def one(cols):
            rows = tokz[z, :, cols] if mine(d) else ztok[d, :, cols]
            stok[d, :, cols] = jnp.dot(sel, rows, preferred_element_type=f32).astype(bf16)

        columns(features, one, features)
        to_peers(lambda k: plane_copy(0, d, k))
        tok_in[chunk_rows(d, own), :] = stok[d, rows_of(own), :]

    def send_cot(d):
        for b in range(tc):
            sel = picker(mbuf[d, b], chunk, group_rows)
            rows = slice(b * group_rows, (b + 1) * group_rows)
            value = cotz[z, rows, :] if mine(d) else zcot[d, rows, :]
            value = jnp.dot(sel, value, preferred_element_type=f32).astype(bf16)
            for q in range(plane_size):
                scot[d, q, b * slots : (b + 1) * slots, :] = value[q * slots : (q + 1) * slots]
        to_peers(lambda k: plane_copy(1, d, k))
        src, dst = plane_parts(1, d, own)
        dst[...] = src[...]

    eye = iota((block, block), 0) == iota((block, block), 1)
    before = iota((block, block), 0) < iota((block, block), 1)

    def column(row):
        return jnp.sum(jnp.where(eye, row, 0.0), axis=1, keepdims=True)

    def count(mask):
        return jnp.sum(mask.astype(f32), axis=0, keepdims=True)

    loads[0].wait()
    loads[1].wait()
    ids = route_ref[...].astype(f32)
    ids = [ids[i : i + 1] for i in range(2)]
    id_cols = [column(row) for row in ids]
    group = sum((ids[0] >= float(g * plane_size)).astype(f32) for g in range(1, zc))
    z_slot = group * group_rows + count((column(group) == group) & before)
    ranks = [
        count((id_cols[0] == ids[0]) & before),
        count(id_cols[0] == ids[1]) + count((id_cols[1] == ids[1]) & before),
    ]
    values = [(ids[i] - group * plane_size) * slots + ranks[i] + 1.0 for i in range(2)]
    values += [gate_ref[i : i + 1].astype(bf16).astype(f32) for i in range(2)]
    value_cols = [column(row) for row in values]
    slot_col = column(z_slot)
    lane = iota((block, block), 1).astype(f32)
    for g in range(zc):
        hit = (slot_col == lane + float(g * group_rows)) & (lane < float(group_rows))
        for i in range(4):
            row = jnp.sum(jnp.where(hit, value_cols[i], 0.0), axis=0, keepdims=True)
            meta[g, i : i + 1, :] = row - 1.0 if i < 2 else row
        meta[g, 4:8, :] = jnp.broadcast_to(z_slot, (4, block))

    def packer(row):
        slot = iota((zc * group_rows, block), 0).astype(f32)
        return (slot == row).astype(f32).astype(bf16)

    own_pack = packer(z_slot)
    loads[2].wait()

    def pack_tokens(cols):
        value = jnp.dot(own_pack, tok[:, cols], preferred_element_type=f32).astype(bf16)
        for g in range(zc):
            tokz[g, :, cols] = value[g * group_rows : (g + 1) * group_rows]

    columns(features, pack_tokens, features)
    everyone()

    for d in range(zc):
        each(0 if d else 1, tc, lambda k: meta_copy(d, k).start())
    for d in sending:
        z_copy(0, d).start()
    mbuf[0, t] = meta[z]

    for load in loads[6:]:
        load.start()
    for load in loads[3:6]:
        load.wait()
    gain = gain_ref[...]
    for b in range(tc):
        rows = slice(b * block, (b + 1) * block)
        saved = saved_ref[rows, :].astype(f32)
        scaled = gain * grad_ref[rows, :].astype(f32)
        for i, value in enumerate((saved * saved, saved * scaled)):
            total = jnp.sum(value, axis=1, keepdims=True)
            row = i * tc + b
            stat[row : row + 1, :] = jnp.sum(jnp.where(eye, total, 0.0), axis=0, keepdims=True)
    each(1, tc, lambda k: stat_copy(k).start())

    send_tok(0)

    each(1, tc, lambda k: stat_copy(k).wait_recv())
    each(1, tc, lambda k: meta_copy(0, k).wait_recv())
    totals = stat[...]
    for k in range(1, tc):
        totals = totals + stbuf[k]
    inv = lax.rsqrt(totals[:tc] / features + epsilon)
    coef = inv * inv * inv * totals[tc:] / features
    for b in range(tc):
        rows = slice(b * block, (b + 1) * block)
        saved = saved_ref[rows, :].astype(f32)
        scaled = gain * grad_ref[rows, :].astype(f32)
        cot = (column(inv[b : b + 1]) * scaled - saved * column(coef[b : b + 1])).astype(bf16)
        packed = jnp.dot(packer(mbuf[0, b, 4:5, :]), cot, preferred_element_type=f32).astype(bf16)
        for g in range(zc):
            cotz[g, b * group_rows : (b + 1) * group_rows, :] = packed[g * group_rows : (g + 1) * group_rows]
    for d in sending:
        z_copy(1, d).start()
    send_cot(0)

    for d in range(1, zc):
        each(0, tc, lambda k: meta_copy(d, k).wait_recv())
    weights = jnp.zeros((chunk, LANES), f32)
    for d in range(zc):
        tile = mbuf[d, t]
        total = jnp.zeros((chunk, 1), f32)
        for i in range(2):
            hit = chosen(tile, i, chunk, group_rows)
            total = total + jnp.sum(
                jnp.where(hit, tile[2 + i : 3 + i, :group_rows], 0.0), axis=1, keepdims=True
            )
        weights = jnp.where(iota((chunk, LANES), 1) == d, total, weights)
    wsend[...] = weights.astype(bf16)
    to_peers(w_copy)
    wrecv[rows_of(own)] = wsend[rows_of(own)]

    def weight_of(d):
        tile = wrecv[...].astype(f32)
        return jnp.sum(jnp.where(iota(tile.shape, 1) == d, tile, 0.0), axis=1, keepdims=True)

    def compute(d):
        rows = whole(d)
        weight = weight_of(d)
        each(1, plane_size, lambda k: plane_copy(0, d, k).wait_recv())
        pre_gate = jnp.dot(tok_in[rows, :], wg[...], preferred_element_type=f32)
        pre_up = jnp.dot(tok_in[rows, :], wu[...], preferred_element_type=f32)
        each(1, plane_size, lambda k: plane_copy(1, d, k).wait_recv())
        hid_grad = contract(cot_in[rows, :], wd[...], 1, 1)
        sigmoid = jax.nn.sigmoid(pre_gate)
        activated = pre_gate * sigmoid
        hidden = activated * pre_up
        d_hidden = weight * hid_grad
        hid[rows, :] = hidden.astype(bf16)
        dg[rows, :] = (d_hidden * pre_up * sigmoid * (1.0 + pre_gate * (1.0 - sigmoid))).astype(bf16)
        du[rows, :] = (d_hidden * activated).astype(bf16)
        total = jnp.sum(hidden * hid_grad, axis=1, keepdims=True)

        def backward(cols):
            value = contract(dg[rows, :], wg[cols, :], 1, 1) + contract(du[rows, :], wu[cols, :], 1, 1)
            back[d, :, cols] = value.astype(bf16)
            cot_in[rows, cols] = (weight * cot_in[rows, cols].astype(f32)).astype(bf16)

        columns(features, backward, features)
        return total

    def give_back(d, piece=0):
        to_peers(lambda k: return_copy(d, k, piece))
        rbuf[d, rows_of(own)] = back[d, rows_of(own)]

    def unite(d):
        each(1, plane_size, lambda k: return_copy(d, k).wait_recv())
        if mine(d):
            each(1, plane_size, lambda k: return_copy(d, k, 1).wait_recv())
        sel = picker(mbuf[d, t], chunk, group_rows)

        def one(cols):
            value = contract(sel, rbuf[d, :, cols], 0, 0).astype(bf16)
            if mine(d):
                land[own_land, cols] = value
            else:
                cbuf[d, :, cols] = value

        columns(features, one, features)
        if not mine(d):
            out_copy(d).start()

    def weight_grad(out, left, right):
        step = min(256, out.shape[0])

        def one(c):
            cols = pl.ds(pl.multiple_of(c * step, step), step)
            out[cols, :] = contract(left[:, cols], right[...], 0, 0).astype(bf16)

        each(0, out.shape[0] // step, one)

    def take(a, d):
        z_copy(a, d).wait_recv()
        if a == 0:
            send_tok(d)
        else:
            send_cot(d)

    def note(tile, d):
        return jnp.where(iota((chunk, LANES), 1) == d, compute(d), tile)

    take(0, early)
    take(0, middle)
    for load in loads[6:]:
        load.wait()
    each(1, plane_size, lambda k: w_copy(k).wait_recv())
    tile = note(jnp.zeros((chunk, LANES), f32), 0)
    take(1, early)
    take(1, middle)
    take(0, late)
    tile = note(tile, early)
    take(1, late)
    tile = note(tile, middle)
    give_back(far)
    tile = note(tile, late)
    ggsend[...] = tile.astype(bf16)
    to_peers(gg_copy)
    ggbuf[rows_of(own)] = ggsend[rows_of(own)]
    give_back(late)
    give_back(near)
    give_back(0)
    give_back(0, 1)
    unite(far)
    weight_grad(dwg_ref, tok_in, dg)
    each(1, plane_size, lambda k: gg_copy(k).wait_recv())
    returned = ggbuf[...].astype(f32)
    for d in range(zc):
        picked = jnp.sum(jnp.where(iota(returned.shape, 1) == d, returned, 0.0), axis=1, keepdims=True)
        for i in range(2):
            hit = chosen(mbuf[d, t], i, chunk, LANES)
            gbuf[d, i : i + 1, :] = jnp.sum(jnp.where(hit, picked, 0.0), axis=0, keepdims=True)
        if d:
            gz_copy(d).start()
    gland[z] = gbuf[0]
    unite(late)
    weight_grad(dwu_ref, tok_in, du)
    unite(near)
    weight_grad(dwd_ref, hid, cot_in)
    for d in range(zc):
        each(0 if d else 1, tc, lambda k: meta_copy(d, k).wait_send())
        for a in range(2):
            each(1, plane_size, lambda k: plane_copy(a, d, k).wait_send())
            if d:
                z_copy(a, d).wait_send()
    each(1, tc, lambda k: stat_copy(k).wait_send())
    each(1, plane_size, lambda k: w_copy(k).wait_send())
    each(1, plane_size, lambda k: gg_copy(k).wait_send())
    for d in range(1, zc):
        gz_copy(d).wait_recv()
    slot_row = mbuf[0, t, 4:5, :]
    outs = []
    for i in range(2):
        row = jnp.zeros((1, block), f32)
        for g in range(zc):
            source = column(gland[g, i : i + 1, :])
            hit = iota((block, block), 0).astype(f32) + float(g * group_rows) == slot_row
            hit = hit & (iota((block, block), 0) < group_rows)
            row = row + jnp.sum(jnp.where(hit, source, 0.0), axis=0, keepdims=True)
        outs.append(row)
    gg_out[...] = jnp.concatenate(outs).astype(bf16)
    unite(0)
    for d in range(1, zc):
        out_copy(d).wait_recv()

    def unpack(cols):
        tg_ref[:, cols] = contract(own_pack, land[:, cols], 0, 0).astype(bf16)

    columns(features, unpack, features)
    for d in range(zc):
        each(1, plane_size, lambda k: return_copy(d, k).wait_send())
        if d == 0:
            each(1, plane_size, lambda k: return_copy(d, k, 1).wait_send())
        if d:
            out_copy(d).wait_send()
            gz_copy(d).wait_send()


def fused_scratch(block, features, part, width, group_rows, zc, tc, plane_size, slots):
    bf16, f32, space = jnp.bfloat16, jnp.float32, pltpu.VMEM
    rows = plane_size * slots
    tile = (META_ROWS, LANES)
    return [
        space((2, block), jnp.int32),
        space((2, block), f32),
        space((1, part), f32),
        space((block, features), bf16),
        space((tc * block, part), bf16),
        space((tc * block, part), bf16),
        space((features, width), bf16),
        space((features, width), bf16),
        space((width, features), bf16),
        space((zc,) + tile, f32),
        space((zc, tc) + tile, f32),
        space((2 * tc, LANES), f32),
        space((tc, 2 * tc, LANES), f32),
        space((zc, group_rows, features), bf16),
        space((zc, tc * group_rows, part), bf16),
        space((zc, group_rows, features), bf16),
        space((zc, tc * group_rows, part), bf16),
        space((zc, rows, features), bf16),
        space((zc, plane_size, tc * slots, part), bf16),
        space((rows, LANES), bf16),
        space((rows, LANES), bf16),
        space((zc * rows, features), bf16),
        space((zc * rows, features), bf16),
        space((zc * rows, width), bf16),
        space((zc * rows, width), bf16),
        space((zc * rows, width), bf16),
        space((zc, rows, features), bf16),
        space((zc, rows, features), bf16),
        space((zc, group_rows, features), bf16),
        space((zc * group_rows, features), bf16),
        space((rows, LANES), bf16),
        space((rows, LANES), bf16),
        space((zc,) + tile, f32),
        space((zc,) + tile, f32),
    ]


def fused(tokens, routes, gates, saved, grad, gain, w_gate, w_up, w_down, scratch, limit, plane_size, slots, zc, tc):
    dma, struct = pltpu.SemaphoreType.DMA, jax.ShapeDtypeStruct
    bf16, f32 = jnp.bfloat16, jnp.float32
    semaphores = [
        dma((9,)),
        dma((zc, tc)),
        dma((zc, tc)),
        dma((tc,)),
        dma((tc,)),
        dma((2, zc)),
        dma((2, zc)),
        dma((2, zc, plane_size)),
        dma((2, zc, plane_size)),
        dma((plane_size,)),
        dma((plane_size,)),
        dma((zc + 1, plane_size)),
        dma((zc + 1, plane_size)),
        dma((zc,)),
        dma((zc,)),
        dma((plane_size,)),
        dma((plane_size,)),
        dma((zc,)),
        dma((zc,)),
    ]
    operands = (tokens, routes, gates, saved, grad, gain, w_gate, w_up, w_down)
    space = pltpu.MemorySpace.HBM
    hbm = pl.BlockSpec(memory_space=space)
    return pl.pallas_call(
        functools.partial(fused_kernel, plane_size, slots),
        out_shape=(
            struct(tokens.shape, bf16),
            struct(routes.shape, bf16),
            struct(w_gate.shape[1:], bf16),
            struct(w_up.shape[1:], bf16),
            struct(w_down.shape[1:], bf16),
        ),
        in_specs=[hbm] * 9,
        out_specs=(vmem(),) * 5,
        scratch_shapes=scratch + semaphores,
        compiler_params=pltpu.CompilerParams(
            collective_id=2, has_side_effects=True, vmem_limit_bytes=limit
        ),
        name="layer",
    )(*(pltpu.with_memory_space_constraint(value, space) for value in operands))


def size_of(refs):
    total = 0
    for ref in refs:
        count = ref.dtype.itemsize if hasattr(ref.dtype, "itemsize") else jnp.dtype(ref.dtype).itemsize
        for extent in ref.shape:
            count *= extent
        total += count
    return total


MIB = 1024 * 1024


def put_kernel(*refs):
    count = len(refs) // 2
    copies = []
    for i in range(count):
        rows = refs[i].shape[0]
        pieces = 4 if rows % 64 == 0 else 1
        for n in range(pieces):
            part = slice(n * rows // pieces, (n + 1) * rows // pieces)
            copies.append(pltpu.make_async_copy(refs[i].at[part], refs[count + i].at[part], refs[-1].at[i, n]))
    for copy in copies:
        copy.start()
    for copy in copies:
        copy.wait()


def put_out(*values):
    return pl.pallas_call(
        put_kernel,
        out_shape=tuple(jax.ShapeDtypeStruct(value.shape, value.dtype) for value in values),
        in_specs=[vmem()] * len(values),
        out_specs=(anywhere(),) * len(values),
        scratch_shapes=[pltpu.SemaphoreType.DMA((len(values), 4))],
        compiler_params=pltpu.CompilerParams(vmem_limit_bytes=MIB),
        name="put",
    )(*values)


def local(tokens, routes, gates, w_gate, w_up, w_down, moe_out, norm_gain, out_grad):
    z_count, x_count, t_count = (lax.axis_size(name) for name in AXES)
    plane_size = x_count * t_count
    tok_rows, features = tokens.shape
    capacity = groups * tok_rows // (z_count * plane_size)
    slots = -(-capacity // 16) * 16
    group_rows = 3 * tok_rows // 8
    scratch = fused_scratch(
        tok_rows, features, moe_out.shape[1], w_gate.shape[2], group_rows, z_count, t_count, plane_size, slots
    )
    held = size_of(scratch)
    grads = 3 * 2 * features * w_gate.shape[2]
    if held + grads + 8 * MIB > 64 * MIB:
        return apart(tokens, routes, gates, w_gate, w_up, w_down, moe_out, norm_gain, out_grad)
    token_grad, rows, grad_gate, grad_up, grad_down = fused(
        tokens,
        routes.T,
        gates.T,
        moe_out,
        out_grad,
        norm_gain[None, :],
        w_gate,
        w_up,
        w_down,
        scratch,
        held + 4 * MIB,
        plane_size,
        slots,
        z_count,
        t_count,
    )
    token_grad, gates_grad, grad_gate, grad_up, grad_down = put_out(
        token_grad, rows, grad_gate, grad_up, grad_down
    )
    return (token_grad, gates_grad.T, grad_gate[None], grad_up[None], grad_down[None])


def solution(mesh):
    ep, tp = mesh.shape["ep"], mesh.shape["tp"]
    cut = Mesh(mesh.devices.reshape(groups, ep // groups, tp), AXES)
    rows, ep_axes = P(AXES, None), ("z", "x")
    cube = P(AXES, None, None)
    return jax.shard_map(
        local,
        mesh=cut,
        in_specs=(rows, rows, rows, cube, cube, cube, P(ep_axes, "tp"), P("tp"), P(ep_axes, "tp")),
        out_specs=(rows, rows, cube, cube, cube),
        check_vma=False,
    )
```
